256 devices in a mesh: sp: 64 (over z, x, core), tp: 4 (over y).
Axes of the slice: x: 4, y: 4, z: 8, core: 2. Of those that a mesh axis runs over, the one named last changes fastest.
Arguments:
- inputs: bfloat16 [32768, 2048], P(('sp', 'tp')), may hold values from -6 to 6
- norm_gain: float32 [2048], replicated, may hold values from 0.1 to 1.9
- w_query: bfloat16 [2048, 1024], P(None, 'tp'), may hold values from -1 to 1
- w_key: bfloat16 [2048, 1024], P(None, 'tp'), may hold values from -1 to 1
- w_value: bfloat16 [2048, 1024], P(None, 'tp'), may hold values from -0.125 to 0.125
- query_gain: float32 [2, 64], replicated, may hold values from 1 to 5.5
- key_gain: float32 [2, 64], replicated, may hold values from 1 to 5.5
- lambdas: float32 [8], P('tp'), may hold values from 0.3 to 0.8
- sub_gain: float32 [128], replicated, may hold values from 0.1 to 1.9
- w_gate_b: bfloat16 [2048, 1024], P(None, 'tp'), may hold values from -0.125 to 0.125
- w_gate_c: bfloat16 [2048, 1024], P(None, 'tp'), may hold values from -0.125 to 0.125
- w_conv_in: bfloat16 [2048, 1024], P(None, 'tp'), may hold values from -0.125 to 0.125
- conv_taps: float32 [3, 1024], P(None, 'tp'), may hold values from -3 to 3
- conv_gain: float32 [1024], P('tp'), may hold values from 0.1 to 1.9
- w_out_att: bfloat16 [1024, 2048], P('tp'), may hold values from -0.125 to 0.125
- w_out_conv: bfloat16 [1024, 2048], P('tp'), may hold values from -0.125 to 0.125
Outputs:
- mixed: float32 [32768, 2048], P(('sp', 'tp'))
- log_sums: float32 [8, 2, 32768], P('tp', None, 'sp')
The draws below stay inside these ranges and needn't reach their ends.
All inputs are finite; a program needn't handle non-finite values.
Results may differ from the reference program's by a relative error of at most 0.034.
Values may be sent and summed in bfloat16 or wider, within the bound.
A program may use at most 192 MiB of HBM per device.

```python
import math
import jax
import jax.numpy as jnp
from jax import lax

D = 2048
ATT_HEADS = 8
QK = 64
VD = 128
CONV = 1024
GROUP = 64
KW = 3
TOKENS = 32768


def draw_query_gain(key, part):
    spread = jax.random.uniform(jax.random.fold_in(key, 11), (2, QK), jnp.float32, -1.0, 1.0)
    return 1.3 * (1.0 + 0.2 * spread)


def draw_key_gain(key, part):
    spread = jax.random.uniform(jax.random.fold_in(key, 23), (2, QK), jnp.float32, -1.0, 1.0)
    return 1.3 * (1.0 + 0.2 * spread)


def projection_pair(key):
    first = jax.random.normal(jax.random.fold_in(key, 101), (D, ATT_HEADS * 2 * QK), jnp.float32)
    second = jax.random.normal(jax.random.fold_in(key, 103), (D, ATT_HEADS * 2 * QK), jnp.float32)
    scale = D ** (-0.5)
    return (jnp.clip(first, -5.0, 5.0) * scale, jnp.clip(second, -5.0, 5.0) * scale)


def draw_w_query(key, part):
    first, second = projection_pair(key)
    return first.astype(jnp.bfloat16)


def draw_w_key(key, part):
    first, second = projection_pair(key)
    return second.astype(jnp.bfloat16)


def draw_inputs(key, part):
    base = jax.random.normal(jax.random.fold_in(key, 201), (TOKENS, D), jnp.float32)
    return jnp.clip(base, -6.0, 6.0).astype(jnp.bfloat16)


def block_levels(own_key, shape, pieces, low, high):
    loudness = 1.0
    for dim, shards_of in pieces:
        draws = jax.random.uniform(jax.random.fold_in(jax.random.fold_in(own_key, 6), dim), (shards_of,), jnp.float32, low / len(pieces), high / len(pieces))
        loudness = loudness * jnp.repeat(jnp.exp(draws), shape[dim] // shards_of).reshape((-1,) + (1,) * (len(shape) - 1 - dim))
    return loudness


def scatter_about(key, shape, deviation, reach, cuts=(), held_as=jnp.bfloat16):
    array = jax.random.normal(key, shape, jnp.float32) * deviation
    if len(cuts) > 0:
        array = block_levels(key, shape, cuts, -0.22, 0.18) * array
    return jnp.clip(array, min=-reach, max=reach).astype(held_as)


def setup_inputs(seed: int = 0) -> dict:
    key_list = jax.random.split(jax.random.key(seed), 17)
    inputs = draw_inputs(jax.random.fold_in(key_list[16], 71), 0)
    norm_gain = jnp.clip(1.0 + 0.18 * jax.random.normal(key_list[1], (D,), jnp.float32), 0.1, 1.9)
    w_query = draw_w_query(jax.random.fold_in(key_list[16], 71), 0)
    w_key = draw_w_key(jax.random.fold_in(key_list[16], 71), 0)
    w_value = scatter_about(key_list[4], (D, ATT_HEADS * VD), D ** -0.5, 0.125, ((1, 4),))
    query_gain = draw_query_gain(jax.random.fold_in(key_list[16], 71), 0)
    key_gain = draw_key_gain(jax.random.fold_in(key_list[16], 71), 0)
    lambdas = jnp.clip(0.3 + 0.5 * jax.random.uniform(key_list[7], (ATT_HEADS,), jnp.float32) ** block_levels(key_list[7], (ATT_HEADS,), ((0, 4),), -0.2, 0.2), 0.3, 0.8)
    sub_gain = jnp.clip(1.0 + 0.18 * jax.random.normal(key_list[8], (VD,), jnp.float32), 0.1, 1.9)
    w_gate_b = scatter_about(key_list[9], (D, CONV), D ** -0.5, 0.125, ((1, 4),))
    w_gate_c = scatter_about(key_list[10], (D, CONV), D ** -0.5, 0.125, ((1, 4),))
    w_conv_in = scatter_about(key_list[11], (D, CONV), D ** -0.5, 0.125, ((1, 4),))
    conv_taps = scatter_about(key_list[12], (KW, CONV), 0.577, 3.0, ((1, 4),), jnp.float32)
    conv_gain = jnp.clip(1.0 + 0.18 * jax.random.normal(key_list[13], (CONV,), jnp.float32), 0.1, 1.9)
    w_out_att = scatter_about(key_list[14], (ATT_HEADS * VD, D), (ATT_HEADS * VD + CONV) ** -0.5, 0.125, ((0, 4),))
    w_out_conv = scatter_about(key_list[15], (CONV, D), (ATT_HEADS * VD + CONV) ** -0.5, 0.125, ((0, 4),))
    return {"inputs": inputs, "norm_gain": norm_gain, "w_query": w_query, "w_key": w_key, "w_value": w_value, "query_gain": query_gain, "key_gain": key_gain, "lambdas": lambdas, "sub_gain": sub_gain, "w_gate_b": w_gate_b, "w_gate_c": w_gate_c, "w_conv_in": w_conv_in, "conv_taps": conv_taps, "conv_gain": conv_gain, "w_out_att": w_out_att, "w_out_conv": w_out_conv}


eps = 1e-06

def rms_scale(values):
    return values * lax.rsqrt(lax.optimization_barrier(jnp.mean(values * values, axis=-1, keepdims=True)) + eps)

def rounded(values):
    return lax.optimization_barrier(values.astype(jnp.bfloat16)).astype(jnp.float32)

def reference(inputs, norm_gain, w_query, w_key, w_value, query_gain, key_gain, lambdas, sub_gain, w_gate_b, w_gate_c, w_conv_in, conv_taps, conv_gain, w_out_att, w_out_conv):
    length = inputs.shape[0]
    normed = (rms_scale(inputs.astype(jnp.float32)) * norm_gain).astype(jnp.bfloat16)

    def project(weight):
        return jnp.dot(normed, weight, preferred_element_type=jnp.float32).astype(jnp.bfloat16)
    query = project(w_query).reshape(length, ATT_HEADS, 2, QK)
    key = project(w_key).reshape(length, ATT_HEADS, 2, QK)
    value = project(w_value).reshape(length, ATT_HEADS, VD)
    qn = (rms_scale(query.astype(jnp.float32)) * query_gain * QK ** (-0.5)).astype(jnp.bfloat16)
    kn = (rms_scale(key.astype(jnp.float32)) * key_gain).astype(jnp.bfloat16)
    keys_f = kn.astype(jnp.float32)
    values_f = value.astype(jnp.float32)
    qblock = math.gcd(length, 128)
    key_pos = jnp.arange(length, dtype=jnp.int32)

    def one_block(start):
        qrows = lax.dynamic_slice_in_dim(qn, start, qblock, 0).astype(jnp.float32)
        scores = jnp.einsum('qhmd,khmd->hmqk', qrows, keys_f)
        query_pos = start + jnp.arange(qblock, dtype=jnp.int32)
        allowed = key_pos[None, :] <= query_pos[:, None]
        scores = jnp.where(allowed, scores, -1e+30)
        top = lax.optimization_barrier(jnp.max(scores, axis=-1, keepdims=True))
        prob = jnp.where(allowed, jnp.exp(scores - top), 0.0)
        total = lax.optimization_barrier(jnp.sum(prob, axis=-1))
        acc = jnp.einsum('hmqk,khd->hmqd', rounded(prob), values_f)
        return (acc / total[..., None], top[..., 0] + jnp.log(total))
    starts = (jnp.arange(length // qblock) * qblock).astype(jnp.int32)
    outs, logs = lax.map(one_block, starts)
    map_out = outs.transpose(1, 2, 0, 3, 4).reshape(ATT_HEADS, 2, length, VD)
    attn = map_out[:, 0] - lambdas[:, None, None] * map_out[:, 1]
    heads_out = (rms_scale(attn) * sub_gain).astype(jnp.bfloat16)
    heads_out = heads_out.transpose(1, 0, 2).reshape(length, ATT_HEADS * VD)
    log_sums = logs.transpose(1, 2, 0, 3).reshape(ATT_HEADS, 2, length)
    gate_b = project(w_gate_b).astype(jnp.float32)
    gate_c = project(w_gate_c).astype(jnp.float32)
    conv_in = project(w_conv_in).astype(jnp.float32)
    u_vals = rounded(gate_c * conv_in)
    padded = jnp.concatenate([jnp.zeros((KW - 1, CONV), jnp.float32), u_vals], axis=0)
    conv = jnp.zeros((length, CONV), jnp.float32)
    for tap in range(KW):
        conv = conv + conv_taps[tap] * padded[tap:tap + length]
    gated = gate_b * conv
    grouped = rms_scale(gated.reshape(length, CONV // GROUP, GROUP)).reshape(length, CONV)
    conv_out = (grouped * conv_gain).astype(jnp.bfloat16)
    mixed = jnp.dot(heads_out, w_out_att, preferred_element_type=jnp.float32)
    mixed = mixed + jnp.dot(conv_out, w_out_conv, preferred_element_type=jnp.float32)
    return (mixed, log_sums)
```

```python
import functools

import jax
import jax.numpy as jnp
from jax import lax
from jax.experimental import pallas as pl
from jax.experimental.pallas import tpu as pltpu
from jax.sharding import PartitionSpec as P


NZ, NX, NY = 8, 4, 4
GROUP = 64
LOG2E = 1.4426950408889634
LN2 = 0.6931471805599453
NEG = -1e30
eps = 1e-06


def rms_scale(values, axis=-1):
    return values * lax.rsqrt(jnp.mean(values * values, axis=axis, keepdims=True) + eps)


def sp_permute(value, target):
    pairs = []
    for z in range(NZ):
        for x in range(NX):
            for c in range(2):
                to = target(z, x, c)
                if to is not None:
                    tz, tx, tc = to
                    pairs.append(((z * NX + x) * 2 + c, ((tz % NZ) * NX + tx % NX) * 2 + tc))
    return lax.ppermute(value, "sp", pairs)


def y_permute(value, by):
    return lax.ppermute(value, "tp", [(i, (i + by) % NY) for i in range(NY)])


def attention_kernel(nb, tq, kb, sub, meta, *refs):
    q_ref = refs[0]
    ks = refs[1 : 1 + nb]
    vs = refs[1 + nb : 1 + 2 * nb]
    m_in, l_in, o_in, m_o, l_o, o_o, kc, w = refs[1 + 2 * nb :]
    t = pl.program_id(0)

    @pl.when(t == 0)
    def _():
        for b in range(nb):
            for m in range(2):
                km = ks[b][:, 64 * m : 64 * m + 64]
                kc[b, m] = jnp.concatenate([km, km], axis=1)

    for m in range(2):
        q = q_ref[0, 64 * m : 64 * m + 64].astype(jnp.float32) * LOG2E
        high = q.astype(jnp.bfloat16)
        w[m, :64] = high
        w[m, 64:] = (q - high.astype(jnp.float32)).astype(jnp.bfloat16)
    m_o[...] = m_in[...]
    l_o[...] = l_in[...]
    o_o[...] = o_in[...]
    items = [(m, j) for m in range(2) for j in range(tq // sub)]

    def scores(b, m, j):
        return jnp.dot(
            kc[b, m], w[m, :, j * sub : (j + 1) * sub], preferred_element_type=jnp.float32
        )

    def run(b, masked, diff):
        s = scores(b, *items[0])
        for i, (m, j) in enumerate(items):
            after = scores(b, *items[i + 1]) if i + 1 < len(items) else None
            if masked:
                d = lax.broadcasted_iota(jnp.int32, s.shape, 0) - lax.broadcasted_iota(
                    jnp.int32, s.shape, 1
                )
                s = jnp.where(d <= diff + j * sub, s, NEG)
            cs = slice(j * sub, (j + 1) * sub)
            m_old = m_o[0, m : m + 1, cs]
            m_new = jnp.maximum(m_old, jnp.max(s, axis=0, keepdims=True))
            a = jnp.exp2(m_old - m_new)
            p = jnp.exp2(s - m_new)
            l_o[0, m : m + 1, cs] = l_o[0, m : m + 1, cs] * a + jnp.sum(p, axis=0, keepdims=True)
            m_o[0, m : m + 1, cs] = m_new
            pv = jnp.dot(vs[b][...], p.astype(jnp.bfloat16), preferred_element_type=jnp.float32)
            o_o[0, m, :, cs] = o_o[0, m, :, cs] * a + pv
            s = after

    for b in range(nb):
        diff = meta[t] - meta[8 + b]

        @pl.when(diff >= kb)
        def _():
            run(b, False, diff)

        @pl.when((diff >= 0) & (diff < kb))
        def _():
            run(b, True, diff)


def attention(meta, qt, ks, vs, state, sub=512):
    m, l, o = state
    nb = len(ks)
    tiles, _, tq = qt.shape
    kb = ks[0].shape[0]

    def whole(shape):
        return pl.BlockSpec(shape, lambda t, meta: (0,) * len(shape))

    def tile(shape):
        return pl.BlockSpec(shape, lambda t, meta: (t,) + (0,) * (len(shape) - 1))

    kept = [tile((1, 2, tq)), tile((1, 2, tq)), tile((1, 2, 128, tq))]
    return pl.pallas_call(
        functools.partial(attention_kernel, nb, tq, kb, sub),
        grid_spec=pltpu.PrefetchScalarGridSpec(
            num_scalar_prefetch=1,
            grid=(tiles,),
            in_specs=[tile((1, 128, tq))] + [whole((kb, 128))] * nb + [whole((128, kb))] * nb + kept,
            out_specs=kept,
            scratch_shapes=[
                pltpu.VMEM((nb, 2, kb, 128), jnp.bfloat16),
                pltpu.VMEM((2, 128, tq), jnp.bfloat16),
            ],
        ),
        out_shape=[jax.ShapeDtypeStruct(a.shape, a.dtype) for a in (m, l, o)],
        input_output_aliases={2 + 2 * nb: 0, 3 + 2 * nb: 1, 4 + 2 * nb: 2},
        cost_estimate=pl.CostEstimate(
            flops=tiles * tq * nb * kb * 2 * 256,
            bytes_accessed=2 * o.size * 4,
            transcendentals=tiles * tq * nb * kb * 2,
        ),
        compiler_params=pltpu.CompilerParams(
            vmem_limit_bytes=56 * 1024 * 1024, dimension_semantics=("arbitrary",)
        ),
    )(meta, qt, *ks, *vs, m, l, o)


def on_device(
    inputs,
    norm_gain,
    w_query,
    w_key,
    w_value,
    query_gain,
    key_gain,
    lambdas,
    sub_gain,
    w_gate_b,
    w_gate_c,
    w_conv_in,
    conv_taps,
    conv_gain,
    w_out_att,
    w_out_conv,
):
    f32, bf16 = jnp.float32, jnp.bfloat16
    sp = lax.axis_index("sp")
    y = lax.axis_index("tp")
    z, x, c = sp // (2 * NX), (sp // 2) % NX, sp % 2
    own = inputs.shape[0]
    rows = own * NY
    heads, comp = lambdas.shape[0], query_gain.shape[1]
    hd = 2 * comp

    normed = (rms_scale(inputs.astype(f32)) * norm_gain).astype(bf16)
    up = y_permute(normed, 1)
    down = y_permute(normed, -1)
    far_a = y_permute(up[: own // 2], 1)
    far_b = y_permute(down[own // 2 :], -1)
    source = jnp.zeros((rows, normed.shape[1]), bf16)
    for block, by, shift in (
        (normed, 0, 0),
        (up, -1, 0),
        (down, 1, 0),
        (far_a, 2, 0),
        (far_b, 2, own // 2),
    ):
        at = ((y + by + NY) % NY) * own + shift
        source = lax.dynamic_update_slice(source, block, (at, jnp.int32(0)))

    def project(weight):
        return jnp.dot(source, weight, preferred_element_type=f32).astype(bf16)

    def project_t(weight):
        return lax.dot_general(
            weight, source, (((0,), (1,)), ((), ())), preferred_element_type=f32
        ).astype(bf16)

    key = project(w_key).reshape(rows, heads, 2, comp)
    kn = (rms_scale(key.astype(f32)) * key_gain).astype(bf16).reshape(rows, heads * hd)
    value_t = project_t(w_value)
    query_t = project_t(w_query).reshape(heads, 2, comp, rows)
    qn_t = rms_scale(query_t.astype(f32), axis=2) * query_gain[None, :, :, None] * comp ** (-0.5)
    qn_t = qn_t.astype(bf16).reshape(heads, hd, rows)

    def partner(value):
        return sp_permute(value, lambda z, x, c: (z, x, 1 - c))

    k_mine = lax.dynamic_slice(kn, (jnp.int32(0), c * hd), (rows, hd))
    k_other = partner(lax.dynamic_slice(kn, (jnp.int32(0), (1 - c) * hd), (rows, hd)))
    v_mine = lax.dynamic_slice(value_t, (c * hd, jnp.int32(0)), (hd, rows))
    v_other = partner(lax.dynamic_slice(value_t, ((1 - c) * hd, jnp.int32(0)), (hd, rows)))
    first = c == 0
    k_own = jnp.concatenate(
        [jnp.where(first, k_mine, k_other), jnp.where(first, k_other, k_mine)], axis=0
    )
    v_own = jnp.concatenate(
        [jnp.where(first, v_mine, v_other), jnp.where(first, v_other, v_mine)], axis=1
    )

    def out_low_high(z, x, c):
        return (z, x, 1) if c == 0 else (NZ - 1 - z, x, 0)

    def out_high(z, x, c):
        return None if c == 0 else (NZ - 1 - z, x, 1)

    got_1 = sp_permute(jnp.where(first, qn_t[1], qn_t[0]), out_low_high)
    got_2 = sp_permute(qn_t[1], out_high)
    q_pair = jnp.stack(
        [jnp.where(first, qn_t[0], got_1), jnp.where(first, got_1, got_2)], axis=0
    )

    def x_permute(value, by):
        return sp_permute(value, lambda z, x, c: (z, x + by, c))

    q_all = jnp.concatenate([q_pair] + [x_permute(q_pair, -r) for r in range(1, NX)], axis=0)

    q_starts = []
    for r in range(NX):
        xr = (x + r) % NX
        q_starts.append(((z * NX + xr) * 2) * rows)
        q_starts.append((((NZ - 1 - z) * NX + xr) * 2 + 1) * rows)

    def k_start(by):
        return (((z + by + NZ) % NZ) * NX + x) * 2 * rows

    def meta(*blocks):
        return jnp.stack(q_starts + [k_start(b) for b in blocks]).astype(jnp.int32)

    def z_permute(value, by):
        return sp_permute(value, lambda z, x, c: (z + by, x, c))

    tiles = 2 * NX
    state = (
        jnp.full((tiles, 2, rows), NEG, f32),
        jnp.zeros((tiles, 2, rows), f32),
        jnp.zeros((tiles, 2, hd, rows), f32),
    )
    k_p, v_p, k_n, v_n = k_own, v_own, k_own, v_own
    state_calls = []
    hops = []
    for step in range(1, NZ // 2):
        k_p, v_p = z_permute(k_p, 1), z_permute(v_p, 1)
        k_n, v_n = z_permute(k_n, -1), z_permute(v_n, -1)
        hops.append((k_p, v_p, k_n, v_n))
    half = rows
    k_far = jnp.concatenate([z_permute(k_p[:half], 1), z_permute(k_n[half:], -1)], axis=0)
    v_far = jnp.concatenate([z_permute(v_p[:, :half], 1), z_permute(v_n[:, half:], -1)], axis=1)
    state = attention(meta(0), q_all, [k_own], [v_own], state)
    for step, (kp, vp, kn_, vn) in enumerate(hops, 1):
        state = attention(meta(-step, step), q_all, [kp, kn_], [vp, vn], state)
    top, total, acc = attention(meta(NZ // 2), q_all, [k_far], [v_far], state)

    stats = jnp.stack([top, total])
    others = [
        jnp.roll(x_permute(stats, -d), 2 * d, axis=1) for d in range(1, NX)
    ]
    m_all = functools.reduce(jnp.maximum, [s[0] for s in others], top)
    t_all = total * jnp.exp2(top - m_all)
    for s in others:
        t_all = t_all + s[1] * jnp.exp2(s[0] - m_all)
    scale = jnp.exp2(top - m_all) / t_all
    log_sums = (m_all[:2] + jnp.log2(t_all[:2])) * LN2
    lam = lax.dynamic_slice(lambdas, (c,), (1,))[0]
    part = (
        acc[:, 0] * scale[:, 0][:, None, :] - acc[:, 1] * (lam * scale[:, 1])[:, None, :]
    ).astype(bf16)
    attn = part[:2].astype(f32)
    for r in range(1, NX):
        attn = attn + x_permute(part[2 * r : 2 * r + 2], r).astype(f32)
    heads_t = (rms_scale(attn, axis=1) * sub_gain[None, :, None]).astype(bf16)

    def back_1(z, x, c):
        return (NZ - 1 - z, x, 1) if c == 0 else (z, x, 0)

    def home(pair):
        one = sp_permute(jnp.where(first, pair[1], pair[0]), back_1)
        two = sp_permute(pair[1], out_high)
        return jnp.stack([jnp.where(first, pair[0], one), jnp.where(first, one, two)])

    heads_home = home(heads_t).reshape(heads * hd, rows)
    log_home = home(log_sums)

    channels = conv_gain.shape[0]
    taps = conv_taps.shape[0]
    gate_b = project(w_gate_b).astype(f32)
    gate_c = project(w_gate_c).astype(f32)
    conv_in = project(w_conv_in).astype(f32)
    u_vals = (gate_c * conv_in).astype(bf16)
    count = NZ * NX * 2
    edge = lax.ppermute(u_vals[rows - (taps - 1) :], "sp", [(i, i + 1) for i in range(count - 1)])
    padded = jnp.concatenate([edge, u_vals], axis=0).astype(f32)
    conv = conv_taps[0] * padded[0:rows]
    for tap in range(1, taps):
        conv = conv + conv_taps[tap] * padded[tap : tap + rows]
    gated = gate_b * conv
    grouped = rms_scale(gated.reshape(rows, channels // GROUP, GROUP)).reshape(rows, channels)
    conv_out = (grouped * conv_gain).astype(bf16)

    mine = lax.dynamic_slice(
        jnp.stack([w_out_att, w_out_conv]),
        (jnp.int32(0), c * hd, jnp.int32(0)),
        (2, hd, w_out_att.shape[1]),
    )
    w_1 = y_permute(mine, 1)
    w_3 = y_permute(mine, -1)
    w_2 = jnp.stack([y_permute(w_1[0], 1), y_permute(w_3[1], -1)])
    gathered = [jnp.stack([w_out_att, w_out_conv])]
    for w in (w_1, w_2, w_3):
        o = partner(w)
        gathered.append(
            jnp.concatenate([jnp.where(first, w, o), jnp.where(first, o, w)], axis=1)
        )
    weights = jnp.concatenate(gathered, axis=0).reshape(-1, w_out_att.shape[1])

    lhs = []
    both = [
        heads_home.reshape(heads * hd, NY, own).transpose(1, 2, 0),
        conv_out.reshape(NY, own, channels),
    ]
    for by in range(NY):
        for block in both:
            piece = lax.dynamic_index_in_dim(block, (y + by) % NY, 0, keepdims=False)
            lhs.append(piece if by == 0 else y_permute(piece, by))
    mixed = jnp.dot(jnp.concatenate(lhs, axis=1), weights, preferred_element_type=f32)
    return (mixed, log_home)


def solution(mesh):
    in_specs = (
        P(("sp", "tp"), None),
        P(),
        P(None, "tp"),
        P(None, "tp"),
        P(None, "tp"),
        P(),
        P(),
        P("tp"),
        P(),
        P(None, "tp"),
        P(None, "tp"),
        P(None, "tp"),
        P(None, "tp"),
        P("tp"),
        P("tp", None),
        P("tp", None),
    )
    out_specs = (P(("sp", "tp"), None), P("tp", None, "sp"))
    return jax.shard_map(
        on_device, mesh=mesh, in_specs=in_specs, out_specs=out_specs, check_vma=False
    )
```

```python
import functools

import jax
import jax.numpy as jnp
from jax import lax
from jax.experimental import pallas as pl
from jax.experimental.pallas import tpu as pltpu
from jax.sharding import PartitionSpec as P


NZ, NX, NY = 8, 4, 4
GROUP = 64
LOG2E = 1.4426950408889634
LN2 = 0.6931471805599453
NEG = -1e30
eps = 1e-06


def rms_scale(values, axis=-1):
    return values * lax.rsqrt(jnp.mean(values * values, axis=axis, keepdims=True) + eps)


def sp_permute(value, target):
    pairs = []
    for z in range(NZ):
        for x in range(NX):
            for c in range(2):
                to = target(z, x, c)
                if to is not None:
                    tz, tx, tc = to
                    pairs.append(((z * NX + x) * 2 + c, ((tz % NZ) * NX + tx % NX) * 2 + tc))
    return lax.ppermute(value, "sp", pairs)


def y_permute(value, by):
    return lax.ppermute(value, "tp", [(i, (i + by) % NY) for i in range(NY)])


MESH = pl.DeviceIdType.MESH
SLOTS = 8


def fused_kernel(
    k_loc,
    v_loc,
    q_loc,
    conv_loc,
    w_att,
    w_conv,
    lam_ref,
    gain_ref,
    a_out,
    log_out,
    cv_out,
    w_out,
    kbuf,
    vbuf,
    qbuf,
    wq,
    acc,
    lsum,
    stats,
    stats_in,
    part,
    part_in,
    heads,
    logs,
    s_send,
    s_recv,
    local_sem,
):
    f32, bf16 = jnp.float32, jnp.bfloat16
    sp = lax.axis_index("sp")
    y = lax.axis_index("tp")
    z = sp // (2 * NX)
    x = lax.rem(sp // 2, NX)
    c = lax.rem(sp, 2)
    zr = NZ - 1 - z
    rows = 512

    def dev(zz, xx, cc, yy):
        return ((zz * NX + xx) * 2 + cc, yy)

    def wrap(v, n):
        return lax.rem(v + n, n)

    z_up, z_dn = wrap(z + 1, NZ), wrap(z - 1, NZ)
    partner = dev(z, x, 1 - c, y)

    barrier = pltpu.get_barrier_semaphore()
    peers = [dev(z_up, x, c, y), dev(z_dn, x, c, y)]
    peers += [dev(z, wrap(x + r, NX), c, y) for r in range(1, NX)]
    for o in range(NY):
        yy = wrap(y + o, NY)
        if o:
            peers.append(dev(z, x, c, yy))
        peers.append(dev(z, x, 1 - c, yy))
        peers.append(dev(zr, x, c, yy))
        peers.append(dev(zr, x, 1 - c, yy))
    for peer in peers:
        pl.semaphore_signal(barrier, inc=1, device_id=peer, device_id_type=MESH)
    pl.semaphore_wait(barrier, len(peers))

    def remote(n, src, dst, to, m=None):
        return pltpu.make_async_remote_copy(
            src_ref=src,
            dst_ref=dst,
            send_sem=s_send.at[n],
            recv_sem=s_recv.at[n if m is None else m],
            device_id=to,
            device_id_type=MESH,
        )

    SWAP, QX, HOP, STAT, PART, HOME, LOGS, CONV, WY, WF, WC = 0, 4, 7, 23, 26, 29, 37, 39, 42, 46, 48

    k_swap = remote(SWAP, k_loc.at[1 - c], kbuf.at[0, c], partner)
    v_swap = remote(SWAP + 1, v_loc.at[1 - c], vbuf.at[0, c], partner)
    q_to = dev(jnp.where(c == 0, z, zr), x, 1 - c, y)
    q_one = remote(SWAP + 2, q_loc.at[1 - c], qbuf.at[c], q_to)
    q_two = remote(SWAP + 3, q_loc.at[1], qbuf.at[1], dev(zr, x, 1, y))
    k_own = pltpu.make_async_copy(k_loc.at[c], kbuf.at[0, c], local_sem.at[0])
    v_own = pltpu.make_async_copy(v_loc.at[c], vbuf.at[0, c], local_sem.at[1])
    q_own = pltpu.make_async_copy(q_loc.at[0], qbuf.at[0], local_sem.at[2])
    k_swap.start()
    v_swap.start()
    q_one.start()
    k_own.start()
    v_own.start()

    @pl.when(c == 0)
    def _():
        q_own.start()

    @pl.when(c == 1)
    def _():
        q_two.start()

    def w_half(ref, cc):
        return ref.at[pl.ds(cc * 128, 128)]

    def w_slot(d, kind, cc):
        return w_out.at[d - 1, kind, pl.ds(cc * 128, 128)]

    y_up, y_dn = dev(z, x, c, wrap(y + 1, NY)), dev(z, x, c, wrap(y - 1, NY))
    w_first = [
        remote(WY, w_half(w_att, c), w_slot(1, 0, c), y_up),
        remote(WY + 1, w_half(w_conv, c), w_slot(1, 1, c), y_up),
        remote(WY + 2, w_half(w_att, c), w_slot(3, 0, c), y_dn),
        remote(WY + 3, w_half(w_conv, c), w_slot(3, 1, c), y_dn),
    ]
    w_far = [
        remote(WF, w_slot(1, 0, c), w_slot(2, 0, c), y_up),
        remote(WF + 1, w_slot(3, 1, c), w_slot(2, 1, c), y_dn),
    ]
    w_core = [
        remote(WC + 2 * (d - 1) + kind, w_slot(d, kind, c), w_slot(d, kind, c), partner)
        for d in range(1, NY)
        for kind in range(2)
    ]
    convs = [
        remote(
            CONV + o - 1,
            conv_loc.at[wrap(y + o, NY)],
            cv_out.at[o],
            dev(z, x, c, wrap(y + o, NY)),
        )
        for o in range(1, NY)
    ]
    cv_own = pltpu.make_async_copy(conv_loc.at[y], cv_out.at[0], local_sem.at[3])
    cv_own.start()
    for copy in convs + w_first:
        copy.start()

    def hop(d):
        out = []
        up, dn = dev(z_up, x, c, y), dev(z_dn, x, c, y)
        for i, buf in enumerate((kbuf, vbuf)):
            n = HOP + 4 * (d - 1) + 2 * i
            a, b = d - 1, (SLOTS - (d - 1)) % SLOTS
            if d < NZ // 2:
                out.append(remote(n, buf.at[a], buf.at[d], up))
                out.append(remote(n + 1, buf.at[b], buf.at[SLOTS - d], dn))
            else:
                out.append(remote(n, buf.at[a, 0], buf.at[d, 0], up))
                out.append(remote(n + 1, buf.at[b, 1], buf.at[d, 1], dn))
        return out

    hops = [None] + [hop(d) for d in range(1, NZ // 2 + 1)]
    q_x = [
        remote(
            QX + r - 1,
            qbuf.at[pl.ds(0, 2)],
            qbuf.at[pl.ds(2 * r, 2)],
            dev(z, wrap(x - r, NX), c, y),
        )
        for r in range(1, NX)
    ]

    wq[...] = jnp.zeros(wq.shape, bf16)
    acc[...] = jnp.zeros(acc.shape, f32)
    lsum[...] = jnp.zeros(lsum.shape, f32)

    def prepare(t):
        for m in range(2):
            q = qbuf[t, 64 * m : 64 * m + 64].astype(f32) * LOG2E
            high = q.astype(bf16)
            wq[t, m, 64 * m : 64 * m + 64] = high
            wq[t, m, 128 + 64 * m : 192 + 64 * m] = (q - high.astype(f32)).astype(bf16)

    def q_start(t):
        r, h = t // 2, lax.rem(t, 2)
        zq = jnp.where(h == 0, z, zr)
        return ((zq * NX + wrap(x + r, NX)) * 2 + h) * rows

    def scoped(s_acc, o_acc):
        def run(t, slots, masked, diff):
            its = [(s, m, g) for m in range(2) for s in slots for g in range(4)]
            n = len(its)
            lag, bufs = 2, 3

            def start(i):
                s, m, g = its[i]
                k = kbuf[s, g // 2, (g % 2) * 256 : (g % 2) * 256 + 256]
                lhs = jnp.concatenate([k, k], axis=1)
                for j in range(2):
                    pltpu.matmul_push_rhs(
                        wq[t, m, :, j * 256 : (j + 1) * 256], staging_register=0, mxu_index=j
                    )
                    pltpu.matmul_acc_lhs(s_acc[j][i % bufs], lhs, load_staged_rhs=0)

            ls = [None, None]
            for i in range(lag):
                start(i)
            for i in range(n):
                s, m, g = its[i]
                if i + lag < n:
                    start(i + lag)
                for j in range(2):
                    sc = pltpu.matmul_pop(s_acc[j][i % bufs])
                    if masked:
                        d = lax.broadcasted_iota(jnp.int32, sc.shape, 0) - lax.broadcasted_iota(
                            jnp.int32, sc.shape, 1
                        )
                        sc = jnp.where(d <= diff + (j * 256 - g * 256), sc, NEG)
                    p = jnp.exp2(sc)
                    one = jnp.sum(p.reshape(32, 8, 256), axis=0)
                    ls[j] = one if ls[j] is None else ls[j] + one
                    pltpu.matmul_push_rhs(p.astype(bf16), staging_register=1, mxu_index=j)
                    pltpu.matmul_acc_lhs(
                        o_acc[j],
                        vbuf[s, g // 2, :, (g % 2) * 256 : (g % 2) * 256 + 256],
                        load_staged_rhs=1,
                    )
                if i + 1 == n or its[i + 1][1] != m:
                    for j in range(2):
                        cs = slice(j * 256, (j + 1) * 256)
                        acc[t, m, :, cs] += pltpu.matmul_pop(o_acc[j])
                        lsum[t, m, :, cs] += ls[j]
                    ls = [None, None]

        def step(u, carry):
            @pl.when(u == 0)
            def _():
                k_own.wait()
                v_own.wait()
                k_swap.wait()
                v_swap.wait()
                for copy in hops[1]:
                    copy.start()
                q_one.wait()

                @pl.when(c == 0)
                def _():
                    q_own.wait()

                @pl.when(c == 1)
                def _():
                    q_two.wait()

                for copy in q_x:
                    copy.start()
                prepare(0)
                prepare(1)

            for d in range(1, NZ // 2 + 1):

                @pl.when(u == d)
                def _(d=d):
                    for copy in hops[d]:
                        copy.wait_recv()
                    if d < NZ // 2:
                        for copy in hops[d + 1]:
                            copy.start()
                    if d == 2:
                        for copy in w_first:
                            copy.wait_recv()
                        for copy in w_far + w_core[:2] + w_core[4:]:
                            copy.start()
                    if d == 4:
                        for copy in w_far:
                            copy.wait_recv()
                        for copy in w_core[2:4]:
                            copy.start()

            sa, sb = u, lax.rem(SLOTS - u, SLOTS)
            two = (u > 0) & (u < NZ // 2)

            def tile(t, carry):
                @pl.when((u == 0) & (t == 2))
                def _():
                    for copy in q_x:
                        copy.wait_recv()

                    def each(i, carry):
                        prepare(i)
                        return carry

                    lax.fori_loop(2, 2 * NX, each, 0)

                def diff_of(s):
                    zk = wrap(z - s, NZ)
                    return q_start(t) - (zk * NX + x) * 2 * rows

                da, db = diff_of(sa), diff_of(sb)
                full = 2 * rows
                both = two & (da >= full) & (db >= full)

                @pl.when(both)
                def _():
                    run(t, [sa, sb], False, 0)

                @pl.when(jnp.logical_not(both))
                def _():
                    def one(b, carry):
                        s = jnp.where(b == 0, sa, sb)
                        diff = diff_of(s)

                        @pl.when(diff >= full)
                        def _():
                            run(t, [s], False, 0)

                        @pl.when((diff >= 0) & (diff < full))
                        def _():
                            run(t, [s], True, diff)

                        return carry

                    lax.fori_loop(0, jnp.where(two, 2, 1), one, 0)

                return carry

            lax.fori_loop(0, 2 * NX, tile, 0)
            return carry

        lax.fori_loop(0, NZ // 2 + 1, step, 0)

    def made(q, count):
        return pltpu.ACC(q)((count, 256), f32)

    pl.run_scoped(
        scoped, [[made(q, 256) for _ in range(3)] for q in range(2)], [made(q, 128) for q in range(2)]
    )

    for t in range(2 * NX):
        for m in range(2):
            stats[t, m : m + 1] = jnp.sum(lsum[t, m], axis=0, keepdims=True)
    st = [
        remote(STAT + r - 1, stats, stats_in.at[r - 1], dev(z, wrap(x - r, NX), c, y))
        for r in range(1, NX)
    ]
    for copy in st:
        copy.start()
    for copy in st:
        copy.wait_recv()
    lam = lam_ref[c]

    def total(t):
        out = stats[t]
        for r in range(1, NX):
            out = out + stats_in[r - 1, (t - 2 * r) % (2 * NX)]
        return out

    def partial(t):
        tot = total(t)
        return acc[t, 0] * (1.0 / tot[0:1]) - acc[t, 1] * (lam / tot[1:2])

    sends = []
    for r in (2, 1, 3):
        for h in range(2):
            part[2 * r + h] = partial(2 * r + h).astype(bf16)
        copy = remote(
            PART + r - 1, part.at[pl.ds(2 * r, 2)], part_in.at[r - 1], dev(z, wrap(x + r, NX), c, y)
        )
        copy.start()
        sends.append(copy)
    for h in range(2):
        acc[h, 0] = partial(h)
        logs[h] = jnp.log(total(h))
    for copy in sends:
        copy.wait_recv()

    homes = []
    for h in range(2):
        attn = acc[h, 0]
        for r in range(1, NX):
            attn = attn + part_in[r - 1, h].astype(f32)
        mean = jnp.mean(attn * attn, axis=0, keepdims=True)
        heads_t = (attn * lax.rsqrt(mean + eps) * gain_ref[...]).astype(bf16)
        for yy in range(NY):
            heads[h, yy] = heads_t[:, yy * 128 : (yy + 1) * 128]
    zh = (z, zr)
    own_head = pltpu.make_async_copy(heads.at[0, y], a_out.at[0], local_sem.at[4])
    own_log = pltpu.make_async_copy(logs.at[0], log_out.at[c], local_sem.at[5])
    late = []
    for h in range(2):
        for o in range(NY):
            yy = wrap(y + o, NY)
            copy = pltpu.make_async_remote_copy(
                src_ref=heads.at[h, yy],
                dst_ref=a_out.at[2 * o + c],
                send_sem=s_send.at[HOME + 4 * h + o],
                recv_sem=s_recv.at[HOME + 2 * o + c],
                device_id=dev(zh[h], x, h, yy),
                device_id_type=MESH,
            )
            if h == 0 and o == 0:
                first = copy
            else:
                copy.start()
                late.append(copy)
        copy = pltpu.make_async_remote_copy(
            src_ref=logs.at[h],
            dst_ref=log_out.at[c],
            send_sem=s_send.at[LOGS + h],
            recv_sem=s_recv.at[LOGS + c],
            device_id=dev(zh[h], x, h, y),
            device_id_type=MESH,
        )
        if h == 0:
            first_log = copy
        else:
            copy.start()
            late.append(copy)

    @pl.when(c == 0)
    def _():
        own_head.start()
        own_log.start()

    @pl.when(c == 1)
    def _():
        first.start()
        first_log.start()

    k_swap_sends = []
    for d in range(1, NZ // 2 + 1):
        k_swap_sends += hops[d]
    for copy in k_swap_sends + q_x + st + sends + late:
        copy.wait_send()
    for copy in w_first + w_far:
        copy.wait_send()
    for copy in w_core + convs:
        copy.wait()
    cv_own.wait()
    for s in range(2 * NY):

        @pl.when((c == 1) | (s > 0))
        def _(s=s):
            remote(HOME, heads.at[0, 0], a_out.at[s], partner, HOME + s).wait_recv()

    for s in range(2):

        @pl.when((c == 1) | (s == 1))
        def _(s=s):
            remote(LOGS, logs.at[0], log_out.at[s], partner, LOGS + s).wait_recv()

    @pl.when(c == 0)
    def _():
        own_head.wait()
        own_log.wait()

    @pl.when(c == 1)
    def _():
        first.wait_send()
        first_log.wait_send()


def fast_attention(kn, value_t, qn_t, conv_out, w_att, w_conv, lambdas, sub_gain):
    f32, bf16 = jnp.float32, jnp.bfloat16
    rows = kn.shape[1]
    vm = pl.BlockSpec(memory_space=pltpu.VMEM)
    hbm = pl.BlockSpec(memory_space=pltpu.HBM)
    sm = pl.BlockSpec(memory_space=pltpu.SMEM)
    tiles = 2 * NX
    return pl.pallas_call(
        fused_kernel,
        in_specs=[vm, vm, vm, vm, hbm, hbm, sm, vm],
        out_specs=[vm, vm, vm, hbm],
        out_shape=[
            jax.ShapeDtypeStruct((2 * NY, 128, 128), bf16),
            jax.ShapeDtypeStruct((2, 2, rows), f32),
            jax.ShapeDtypeStruct((NY, rows // NY, conv_out.shape[2]), bf16),
            jax.ShapeDtypeStruct((NY - 1, 2, *w_att.shape), bf16),
        ],
        scratch_shapes=[
            pltpu.VMEM((SLOTS, 2, rows, 128), bf16),
            pltpu.VMEM((SLOTS, 2, 128, rows), bf16),
            pltpu.VMEM((tiles, 128, rows), bf16),
            pltpu.VMEM((tiles, 2, 256, rows), bf16),
            pltpu.VMEM((tiles, 2, 128, rows), f32),
            pltpu.VMEM((tiles, 2, 8, rows), f32),
            pltpu.VMEM((tiles, 2, rows), f32),
            pltpu.VMEM((NX - 1, tiles, 2, rows), f32),
            pltpu.VMEM((tiles, 128, rows), bf16),
            pltpu.VMEM((NX - 1, 2, 128, rows), bf16),
            pltpu.VMEM((2, NY, 128, 128), bf16),
            pltpu.VMEM((2, 2, rows), f32),
            pltpu.SemaphoreType.DMA((54,)),
            pltpu.SemaphoreType.DMA((54,)),
            pltpu.SemaphoreType.DMA((6,)),
        ],
        cost_estimate=pl.CostEstimate(
            flops=2 * 10**10, bytes_accessed=16 * 2**20, transcendentals=34 * 10**6
        ),
        compiler_params=pltpu.CompilerParams(
            collective_id=1, has_side_effects=True, vmem_limit_bytes=56 * 1024 * 1024
        ),
    )(kn, value_t, qn_t, conv_out, w_att, w_conv, lambdas, sub_gain)


def gather_kernel(x_ref, out, s_send, s_recv, local_sem):
    sp = lax.axis_index("sp")
    y = lax.axis_index("tp")
    up, dn = lax.rem(y + 1, NY), lax.rem(y + NY - 1, NY)
    barrier = pltpu.get_barrier_semaphore()
    for peer in (up, dn):
        pl.semaphore_signal(barrier, inc=1, device_id=(sp, peer), device_id_type=MESH)
    pl.semaphore_wait(barrier, 2)
    half = x_ref.shape[0] // 2

    def part(ref, h):
        return ref.at[pl.ds(h * half, half)]

    def remote(n, src, dst, to):
        return pltpu.make_async_remote_copy(
            src_ref=src,
            dst_ref=dst,
            send_sem=s_send.at[n],
            recv_sem=s_recv.at[n],
            device_id=(sp, to),
            device_id_type=MESH,
        )

    own = pltpu.make_async_copy(x_ref, out.at[y], local_sem)
    one = [
        remote(0, part(x_ref, 0), part(out.at[y], 0), up),
        remote(1, part(x_ref, 1), part(out.at[y], 1), dn),
        remote(2, part(x_ref, 1), part(out.at[y], 1), up),
        remote(3, part(x_ref, 0), part(out.at[y], 0), dn),
    ]
    for copy in one:
        copy.start()
    own.start()
    far = [
        remote(4, part(out.at[dn], 0), part(out.at[dn], 0), up),
        remote(5, part(out.at[up], 1), part(out.at[up], 1), dn),
    ]
    one[0].wait_recv()
    far[0].start()
    one[1].wait_recv()
    far[1].start()
    one[2].wait_recv()
    one[3].wait_recv()
    for copy in far:
        copy.wait()
    for copy in one:
        copy.wait_send()
    own.wait()


def gather_rows(normed):
    rows, width = normed.shape
    return pl.pallas_call(
        gather_kernel,
        in_specs=[pl.BlockSpec(memory_space=pltpu.VMEM)],
        out_specs=pl.BlockSpec(memory_space=pltpu.VMEM),
        out_shape=jax.ShapeDtypeStruct((NY, rows, width), normed.dtype),
        scratch_shapes=[
            pltpu.SemaphoreType.DMA((6,)),
            pltpu.SemaphoreType.DMA((6,)),
            pltpu.SemaphoreType.DMA,
        ],
        compiler_params=pltpu.CompilerParams(collective_id=0, has_side_effects=True),
    )(normed).reshape(NY * rows, width)


def mix_kernel(a_ref, cv_ref, wa, wc, wo, out, a_rows):
    @pl.when(pl.program_id(0) == 0)
    def _():
        for s in range(2 * NY):
            a_rows[:, s * 128 : (s + 1) * 128] = a_ref[s].T

    total = jnp.dot(a_rows[:, :256], wa[...], preferred_element_type=jnp.float32)
    total += jnp.dot(cv_ref[0], wc[...], preferred_element_type=jnp.float32)
    for d in range(1, NY):
        total += jnp.dot(
            a_rows[:, d * 256 : (d + 1) * 256], wo[d - 1, 0], preferred_element_type=jnp.float32
        )
        total += jnp.dot(cv_ref[d], wo[d - 1, 1], preferred_element_type=jnp.float32)
    out[...] = total


def mix(a, cv, w_att, w_conv, w_others):
    own, width, tile = a.shape[2], w_att.shape[1], 512
    return pl.pallas_call(
        mix_kernel,
        grid=(width // tile,),
        in_specs=[
            pl.BlockSpec(a.shape, lambda n: (0, 0, 0)),
            pl.BlockSpec(cv.shape, lambda n: (0, 0, 0)),
            pl.BlockSpec((w_att.shape[0], tile), lambda n: (0, n)),
            pl.BlockSpec((w_conv.shape[0], tile), lambda n: (0, n)),
            pl.BlockSpec((*w_others.shape[:3], tile), lambda n: (0, 0, 0, n)),
        ],
        out_specs=pl.BlockSpec((own, tile), lambda n: (0, n)),
        out_shape=jax.ShapeDtypeStruct((own, width), jnp.float32),
        scratch_shapes=[pltpu.VMEM((own, 1024), jnp.bfloat16)],
        cost_estimate=pl.CostEstimate(
            flops=2 * own * 2048 * width, bytes_accessed=9 * 2**20, transcendentals=0
        ),
        compiler_params=pltpu.CompilerParams(dimension_semantics=("arbitrary",)),
    )(a, cv, w_att, w_conv, w_others)


def online_kernel(meta, q_ref, k_ref, v_ref, m_o, l_o, o_o):
    t, b = pl.program_id(0), pl.program_id(1)
    f32 = jnp.float32
    kb, tq, sub = k_ref.shape[1], q_ref.shape[2], 256

    @pl.when(b == 0)
    def _():
        m_o[...] = jnp.full(m_o.shape, NEG, f32)
        l_o[...] = jnp.zeros(l_o.shape, f32)
        o_o[...] = jnp.zeros(o_o.shape, f32)

    diff = meta[t] - meta[2 * NX + b]

    @pl.when(diff >= 0)
    def _():
        for m in range(2):
            for j in range(tq // sub):
                cs = slice(j * sub, (j + 1) * sub)
                s = jnp.dot(
                    k_ref[0, :, 64 * m : 64 * m + 64],
                    q_ref[0, 64 * m : 64 * m + 64, cs],
                    preferred_element_type=f32,
                )
                d = lax.broadcasted_iota(jnp.int32, s.shape, 0) - lax.broadcasted_iota(
                    jnp.int32, s.shape, 1
                )
                s = jnp.where(d <= diff + j * sub, s, NEG)
                m_old = m_o[0, m : m + 1, cs]
                m_new = jnp.maximum(m_old, jnp.max(s, axis=0, keepdims=True))
                a = jnp.exp(m_old - m_new)
                p = jnp.exp(s - m_new)
                l_o[0, m : m + 1, cs] = l_o[0, m : m + 1, cs] * a + jnp.sum(
                    p, axis=0, keepdims=True
                )
                m_o[0, m : m + 1, cs] = m_new
                pv = jnp.dot(v_ref[0], p.astype(jnp.bfloat16), preferred_element_type=f32)
                o_o[0, m, :, cs] = o_o[0, m, :, cs] * a + pv


def online_attention(meta, q, k, v):
    tiles, _, tq = q.shape
    blocks, kb, hd = k.shape
    f32 = jnp.float32
    return pl.pallas_call(
        online_kernel,
        grid_spec=pltpu.PrefetchScalarGridSpec(
            num_scalar_prefetch=1,
            grid=(tiles, blocks),
            in_specs=[
                pl.BlockSpec((1, hd, tq), lambda t, b, meta: (t, 0, 0)),
                pl.BlockSpec((1, kb, hd), lambda t, b, meta: (b, 0, 0)),
                pl.BlockSpec((1, hd, kb), lambda t, b, meta: (b, 0, 0)),
            ],
            out_specs=[
                pl.BlockSpec((1, 2, tq), lambda t, b, meta: (t, 0, 0)),
                pl.BlockSpec((1, 2, tq), lambda t, b, meta: (t, 0, 0)),
                pl.BlockSpec((1, 2, hd, tq), lambda t, b, meta: (t, 0, 0, 0)),
            ],
        ),
        out_shape=[
            jax.ShapeDtypeStruct((tiles, 2, tq), f32),
            jax.ShapeDtypeStruct((tiles, 2, tq), f32),
            jax.ShapeDtypeStruct((tiles, 2, hd, tq), f32),
        ],
        compiler_params=pltpu.CompilerParams(
            vmem_limit_bytes=56 * 1024 * 1024, dimension_semantics=("arbitrary", "arbitrary")
        ),
    )(meta, q, k, v)


def general_attention(kn, value_t, qn_t, conv, w_att, w_conv, lambdas, sub_gain):
    f32, bf16 = jnp.float32, jnp.bfloat16
    sp = lax.axis_index("sp")
    y = lax.axis_index("tp")
    z, x, c = sp // (2 * NX), (sp // 2) % NX, sp % 2
    heads, rows, hd = kn.shape
    first = c == 0

    def partner(value):
        return sp_permute(value, lambda z, x, c: (z, x, 1 - c))

    def swapped(value, axis):
        mine = jnp.where(first, value[0], value[1])
        other = partner(jnp.where(first, value[1], value[0]))
        return jnp.concatenate(
            [jnp.where(first, mine, other), jnp.where(first, other, mine)], axis=axis
        )

    k_own, v_own = swapped(kn, 0), swapped(value_t, 1)

    def out_one(z, x, c):
        return (z, x, 1) if c == 0 else (NZ - 1 - z, x, 0)

    def out_two(z, x, c):
        return None if c == 0 else (NZ - 1 - z, x, 1)

    got_1 = sp_permute(jnp.where(first, qn_t[1], qn_t[0]), out_one)
    got_2 = sp_permute(qn_t[1], out_two)
    q_pair = jnp.stack([jnp.where(first, qn_t[0], got_1), jnp.where(first, got_1, got_2)], axis=0)

    def x_permute(value, by):
        return sp_permute(value, lambda z, x, c: (z, x + by, c))

    q_all = jnp.concatenate([q_pair] + [x_permute(q_pair, -r) for r in range(1, NX)], axis=0)
    q_starts = []
    for r in range(NX):
        xr = (x + r) % NX
        q_starts.append(((z * NX + xr) * 2) * rows)
        q_starts.append((((NZ - 1 - z) * NX + xr) * 2 + 1) * rows)
    k_starts = [(((z - b + NZ) % NZ) * NX + x) * 2 * rows for b in range(NZ)]
    meta = jnp.stack(q_starts + k_starts).astype(jnp.int32)
    ks, vs = [k_own], [v_own]
    for _ in range(NZ - 1):
        ks.append(sp_permute(ks[-1], lambda z, x, c: (z + 1, x, c)))
        vs.append(sp_permute(vs[-1], lambda z, x, c: (z + 1, x, c)))
    top, total, acc = online_attention(meta, q_all, jnp.stack(ks), jnp.stack(vs))

    stats = jnp.stack([top, total])
    others = [jnp.roll(x_permute(stats, -d), 2 * d, axis=1) for d in range(1, NX)]
    m_all = functools.reduce(jnp.maximum, [s[0] for s in others], top)
    t_all = total * jnp.exp(top - m_all)
    for s in others:
        t_all = t_all + s[1] * jnp.exp(s[0] - m_all)
    scale = jnp.exp(top - m_all) / t_all
    log_sums = m_all[:2] + jnp.log(t_all[:2])
    lam = lax.dynamic_slice(lambdas, (c,), (1,))[0]
    part = acc[:, 0] * scale[:, 0][:, None, :] - acc[:, 1] * (lam * scale[:, 1])[:, None, :]
    attn = part[:2]
    part = part.astype(bf16)
    for r in range(1, NX):
        attn = attn + x_permute(part[2 * r : 2 * r + 2], r).astype(f32)
    heads_t = (rms_scale(attn, axis=1) * sub_gain[None]).astype(bf16)

    def back(z, x, c):
        return (NZ - 1 - z, x, 1) if c == 0 else (z, x, 0)

    def home(pair):
        one = sp_permute(jnp.where(first, pair[1], pair[0]), back)
        two = sp_permute(pair[1], out_two)
        return jnp.stack([jnp.where(first, pair[0], one), jnp.where(first, one, two)])

    heads_home = home(heads_t).reshape(heads, hd, NY, rows // NY).transpose(2, 0, 1, 3)

    def exchange(value, by):
        piece = lax.dynamic_index_in_dim(value, (y + by) % NY, 0, keepdims=False)
        return piece if by == 0 else y_permute(piece, by)

    a = jnp.concatenate([exchange(heads_home, by) for by in range(NY)], axis=0)
    cv = jnp.stack([exchange(conv, by) for by in range(NY)])
    pair = jnp.stack([w_att, w_conv])
    others = jnp.stack([y_permute(pair, d) for d in range(1, NY)])
    return a, home(log_sums), cv, others


def on_device(
    inputs,
    norm_gain,
    w_query,
    w_key,
    w_value,
    query_gain,
    key_gain,
    lambdas,
    sub_gain,
    w_gate_b,
    w_gate_c,
    w_conv_in,
    conv_taps,
    conv_gain,
    w_out_att,
    w_out_conv,
):
    f32, bf16 = jnp.float32, jnp.bfloat16
    own = inputs.shape[0]
    rows = own * NY
    heads, comp = lambdas.shape[0], query_gain.shape[1]
    hd = 2 * comp

    normed = (rms_scale(inputs.astype(f32)) * norm_gain).astype(bf16)
    source = gather_rows(normed)

    def project(weight):
        return jnp.dot(source, weight, preferred_element_type=f32).astype(bf16)

    def project_t(weight):
        return lax.dot_general(
            weight, source, (((0,), (1,)), ((), ())), preferred_element_type=f32
        ).astype(bf16)

    channels = conv_gain.shape[0]
    taps = conv_taps.shape[0]
    gate_c = project(w_gate_c).astype(f32)
    conv_in = project(w_conv_in).astype(f32)
    u_vals = (gate_c * conv_in).astype(bf16)
    count = NZ * NX * 2
    edge = lax.ppermute(u_vals[rows - (taps - 1) :], "sp", [(i, i + 1) for i in range(count - 1)])

    key = project(w_key).reshape(rows, heads, 2, comp)
    kn = (rms_scale(key.astype(f32)) * key_gain).astype(bf16).reshape(rows, heads, hd)
    kn = kn.transpose(1, 0, 2)
    value_t = project_t(w_value).reshape(heads, hd, rows)
    query_t = project_t(w_query).reshape(heads, 2, comp, rows)
    qn_t = rms_scale(query_t.astype(f32), axis=2) * query_gain[None, :, :, None] * comp ** (-0.5)
    qn_t = qn_t.astype(bf16).reshape(heads, hd, rows)

    gate_b = project(w_gate_b).astype(f32)
    padded = jnp.concatenate([edge, u_vals], axis=0).astype(f32)
    conv = conv_taps[0] * padded[0:rows]
    for tap in range(1, taps):
        conv = conv + conv_taps[tap] * padded[tap : tap + rows]
    gated = gate_b * conv
    grouped = rms_scale(gated.reshape(rows, channels // GROUP, GROUP)).reshape(rows, channels)
    conv_out = (grouped * conv_gain).astype(bf16).reshape(NY, own, channels)

    reach = jnp.max(jnp.abs(query_gain * key_gain)) * (comp**0.5) * LOG2E * 1.02
    a, log_sums, cv, w_others = lax.cond(
        reach < 90.0,
        fast_attention,
        general_attention,
        kn,
        value_t,
        qn_t,
        conv_out,
        w_out_att,
        w_out_conv,
        lambdas,
        sub_gain[:, None],
    )
    return (mix(a, cv, w_out_att, w_out_conv, w_others), log_sums)


def solution(mesh):
    in_specs = (
        P(("sp", "tp"), None),
        P(),
        P(None, "tp"),
        P(None, "tp"),
        P(None, "tp"),
        P(),
        P(),
        P("tp"),
        P(),
        P(None, "tp"),
        P(None, "tp"),
        P(None, "tp"),
        P(None, "tp"),
        P("tp"),
        P("tp", None),
        P("tp", None),
    )
    out_specs = (P(("sp", "tp"), None), P("tp", None, "sp"))
    return jax.shard_map(
        on_device, mesh=mesh, in_specs=in_specs, out_specs=out_specs, check_vma=False
    )
```

```python
import functools

import jax
import jax.numpy as jnp
from jax import lax
from jax.experimental import pallas as pl
from jax.experimental.pallas import tpu as pltpu
from jax.sharding import PartitionSpec as P

NZ, NX, NY = 8, 4, 4
GROUP = 64
LOG2E = 1.4426950408889634
LN2 = 0.6931471805599453
NEG = -1e30
eps = 1e-06


MESH = pl.DeviceIdType.MESH
SLOTS = 8


def front_kernel(
    x_ref,
    ngain_ref,
    qgain_ref,
    kgain_ref,
    wq_ref,
    wk_ref,
    wv_ref,
    wb_ref,
    wc_ref,
    wi_ref,
    k_out,
    v_out,
    q_out,
    u_out,
    gate_out,
    edge_out,
    buf,
    weights,
    gains,
    s_send,
    s_recv,
    w_sem,
):
    f32, bf16 = jnp.float32, jnp.bfloat16
    sp = lax.axis_index("sp")
    y = lax.axis_index("tp")
    count = NZ * NX * 2
    up, dn = lax.rem(y + 1, NY), lax.rem(y + NY - 1, NY)
    after, before = lax.rem(sp + 1, count), lax.rem(sp + count - 1, count)
    w_loads = [
        pltpu.make_async_copy(ref, weights.at[i], w_sem.at[i])
        for i, ref in enumerate((wq_ref, wk_ref, wv_ref, wc_ref, wi_ref, wb_ref))
    ]
    for copy in w_loads:
        copy.start()
    barrier = pltpu.get_barrier_semaphore()
    for peer in ((sp, up), (sp, dn), (after, y), (before, y)):
        pl.semaphore_signal(barrier, inc=1, device_id=peer, device_id_type=MESH)

    own = x_ref.shape[0]
    piece = 16

    def norm(i, carry):
        at = pl.ds(pl.multiple_of(i * piece, piece), piece)
        v = x_ref[at].astype(f32)
        scale = lax.rsqrt(jnp.mean(v * v, axis=1, keepdims=True) + eps)
        buf[y, at] = (v * scale * ngain_ref[...]).astype(bf16)
        return carry

    lax.fori_loop(0, own // piece, norm, 0)
    for i, (ref, scale) in enumerate(((qgain_ref, 0.125), (kgain_ref, 1.0))):
        row = jnp.concatenate([ref[0:1], ref[1:2]], axis=1) * scale
        gains[i] = jnp.broadcast_to(row, (128, 128)).T
    pl.semaphore_wait(barrier, 4)
    half = own // 2

    def part(s, h):
        return buf.at[s, pl.ds(h * half, half)]

    def remote(n, src, dst, to):
        return pltpu.make_async_remote_copy(
            src_ref=src,
            dst_ref=dst,
            send_sem=s_send.at[n],
            recv_sem=s_recv.at[n],
            device_id=to,
            device_id_type=MESH,
        )

    one = [
        remote(0, part(y, 0), part(y, 0), (sp, up)),
        remote(1, part(y, 1), part(y, 1), (sp, dn)),
        remote(2, part(y, 1), part(y, 1), (sp, up)),
        remote(3, part(y, 0), part(y, 0), (sp, dn)),
    ]
    for copy in one:
        copy.start()
    far = [
        remote(4, part(dn, 0), part(dn, 0), (sp, up)),
        remote(5, part(up, 1), part(up, 1), (sp, dn)),
    ]
    rows = u_out.shape[0]
    edge = remote(6, u_out.at[pl.ds(rows - 16, 16)], edge_out, (after, y))
    for copy in w_loads:
        copy.wait()

    def block(i, carry):
        s = lax.rem(y + jnp.where(i == 1, NY - 1, jnp.where(i == 2, 1, jnp.where(i == 3, 2, 0))), NY)

        @pl.when(i == 1)
        def _():
            one[0].wait_recv()
            far[0].start()
            one[1].wait_recv()
            far[1].start()
            one[2].wait_recv()

        @pl.when(i == 2)
        def _():
            one[3].wait_recv()

        @pl.when(i == 3)
        def _():
            for copy in far:
                copy.wait_recv()

        xb = buf[s]
        at = pl.ds(pl.multiple_of(s * own, own), own)

        def project(n):
            return jnp.dot(xb, weights[n], preferred_element_type=f32).astype(bf16).astype(f32)

        def scaled(v):
            r = v.T.reshape(4, 64, own)
            return (r * lax.rsqrt(jnp.mean(r * r, axis=1, keepdims=True) + eps)).reshape(2, 128, own)

        q = scaled(project(0))
        k = scaled(project(1))
        for h in range(2):
            q_out[h, :, at] = (q[h] * gains[0]).astype(bf16)
            k_out[h, at] = (k[h] * gains[1]).T.astype(bf16)
        v = project(2).T.astype(bf16)
        for h in range(2):
            v_out[h, :, at] = v[128 * h : 128 * h + 128]
        u_out[at] = (project(3) * project(4)).astype(bf16)
        gate_out[at] = project(5).astype(bf16)

        @pl.when(s == NY - 1)
        def _():
            edge.start()

        return carry

    lax.fori_loop(0, NY, block, 0)
    edge.wait()
    for copy in one + far:
        copy.wait_send()


def front(inputs, norm_gain, query_gain, key_gain, *weights):
    bf16 = jnp.bfloat16
    own, width = inputs.shape
    rows, cols = NY * own, weights[0].shape[1]
    vm = pl.BlockSpec(memory_space=pltpu.VMEM)
    hbm = pl.BlockSpec(memory_space=pltpu.HBM)
    return pl.pallas_call(
        front_kernel,
        in_specs=[vm] * 4 + [hbm] * 6,
        out_specs=[vm] * 6,
        out_shape=[
            jax.ShapeDtypeStruct((2, rows, 128), bf16),
            jax.ShapeDtypeStruct((2, 128, rows), bf16),
            jax.ShapeDtypeStruct((2, 128, rows), bf16),
            jax.ShapeDtypeStruct((rows, cols), bf16),
            jax.ShapeDtypeStruct((rows, cols), bf16),
            jax.ShapeDtypeStruct((16, cols), bf16),
        ],
        scratch_shapes=[
            pltpu.VMEM((NY, own, width), bf16),
            pltpu.VMEM((6, width, cols), bf16),
            pltpu.VMEM((2, 128, 128), jnp.float32),
            pltpu.SemaphoreType.DMA((7,)),
            pltpu.SemaphoreType.DMA((7,)),
            pltpu.SemaphoreType.DMA((6,)),
        ],
        cost_estimate=pl.CostEstimate(
            flops=2 * rows * width * cols * 6, bytes_accessed=8 * 2**20, transcendentals=0
        ),
        compiler_params=pltpu.CompilerParams(
            collective_id=0, has_side_effects=True, vmem_limit_bytes=63 * 1024 * 1024
        ),
    )(inputs, norm_gain, query_gain, key_gain, *weights)


def fused_kernel(
    general,
    k_loc,
    v_loc,
    q_loc,
    u_ref,
    gate_ref,
    edge_ref,
    taps_ref,
    cgain_ref,
    w_att,
    w_conv,
    lam_ref,
    gain_ref,
    out_ref,
    log_out,
    kbuf,
    vbuf,
    qbuf,
    wq,
    acc,
    lsum,
    stats,
    stats_in,
    part,
    part_in,
    heads,
    logs,
    conv_loc,
    a_in,
    cv_in,
    w_own,
    w_in,
    padded,
    a_rows,
    tops,
    s_send,
    s_recv,
    local_sem,
):
    f32, bf16 = jnp.float32, jnp.bfloat16
    sp = lax.axis_index("sp")
    y = lax.axis_index("tp")
    z = sp // (2 * NX)
    x = lax.rem(sp // 2, NX)
    c = lax.rem(sp, 2)
    zr = NZ - 1 - z
    rows = 512

    def dev(zz, xx, cc, yy):
        return ((zz * NX + xx) * 2 + cc, yy)

    def wrap(v, n):
        return lax.rem(v + n, n)

    z_up, z_dn = wrap(z + 1, NZ), wrap(z - 1, NZ)
    x_up, x_dn = dev(z, wrap(x + 1, NX), c, y), dev(z, wrap(x - 1, NX), c, y)
    partner = dev(z, x, 1 - c, y)

    w_loads = [
        pltpu.make_async_copy(w_att, w_own.at[0], local_sem.at[6]),
        pltpu.make_async_copy(w_conv, w_own.at[1], local_sem.at[7]),
    ]
    for copy in w_loads:
        copy.start()

    barrier = pltpu.get_barrier_semaphore()
    peers = [dev(z_up, x, c, y), dev(z_dn, x, c, y)]
    peers += [dev(z, wrap(x + r, NX), c, y) for r in range(1, NX)]
    for o in range(NY):
        yy = wrap(y + o, NY)
        if o:
            peers.append(dev(z, x, c, yy))
        peers.append(dev(z, x, 1 - c, yy))
        peers.append(dev(zr, x, c, yy))
        peers.append(dev(zr, x, 1 - c, yy))
    for peer in peers:
        pl.semaphore_signal(barrier, inc=1, device_id=peer, device_id_type=MESH)
    pl.semaphore_wait(barrier, len(peers))

    def remote(n, src, dst, to, m=None):
        return pltpu.make_async_remote_copy(
            src_ref=src,
            dst_ref=dst,
            send_sem=s_send.at[n],
            recv_sem=s_recv.at[n if m is None else m],
            device_id=to,
            device_id_type=MESH,
        )

    SWAP, QX, HOP, STAT, PART, HOME, LOGS, CONV, WY, WF, WC = 0, 4, 8, 24, 27, 31, 39, 41, 44, 48, 50

    k_swap = remote(SWAP, k_loc.at[1 - c], kbuf.at[0, c], partner)
    v_swap = remote(SWAP + 1, v_loc.at[1 - c], vbuf.at[0, c], partner)
    q_to = dev(jnp.where(c == 0, z, zr), x, 1 - c, y)
    q_one = remote(SWAP + 2, q_loc.at[1 - c], qbuf.at[c], q_to)
    q_two = remote(SWAP + 3, q_loc.at[1], qbuf.at[1], dev(zr, x, 1, y))
    k_own = pltpu.make_async_copy(k_loc.at[c], kbuf.at[0, c], local_sem.at[0])
    v_own = pltpu.make_async_copy(v_loc.at[c], vbuf.at[0, c], local_sem.at[1])
    q_own = pltpu.make_async_copy(q_loc.at[0], qbuf.at[0], local_sem.at[2])
    q_one.start()

    @pl.when(c == 0)
    def _():
        q_own.start()

    @pl.when(c == 1)
    def _():
        q_two.start()

    k_swap.start()
    v_swap.start()
    k_own.start()
    v_own.start()

    def w_half(kind, cc):
        return w_own.at[kind, pl.ds(cc * 128, 128)]

    def w_slot(d, kind, cc):
        return w_in.at[d - 1, kind, pl.ds(cc * 128, 128)]

    y_up, y_dn = dev(z, x, c, wrap(y + 1, NY)), dev(z, x, c, wrap(y - 1, NY))
    w_first = [
        remote(WY, w_half(0, c), w_slot(1, 0, c), y_up),
        remote(WY + 1, w_half(1, c), w_slot(1, 1, c), y_up),
        remote(WY + 2, w_half(0, c), w_slot(3, 0, c), y_dn),
        remote(WY + 3, w_half(1, c), w_slot(3, 1, c), y_dn),
    ]
    w_far = [
        remote(WF, w_slot(1, 0, c), w_slot(2, 0, c), y_up),
        remote(WF + 1, w_slot(3, 1, c), w_slot(2, 1, c), y_dn),
    ]
    w_core = [
        remote(WC + 2 * (d - 1) + kind, w_slot(d, kind, c), w_slot(d, kind, c), partner)
        for d in range(1, NY)
        for kind in range(2)
    ]
    convs = [
        remote(
            CONV + o - 1,
            conv_loc.at[wrap(y + o, NY)],
            cv_in.at[o],
            dev(z, x, c, wrap(y + o, NY)),
        )
        for o in range(1, NY)
    ]
    cv_own = pltpu.make_async_copy(conv_loc.at[y], cv_in.at[0], local_sem.at[3])

    def hop(d, i):
        out = []
        up, dn = dev(z_up, x, c, y), dev(z_dn, x, c, y)
        buf = (kbuf, vbuf)[i]
        n = HOP + 4 * (d - 1) + 2 * i
        a, b = d - 1, (SLOTS - (d - 1)) % SLOTS
        if d < NZ // 2:
            out.append(remote(n, buf.at[a], buf.at[d], up))
            out.append(remote(n + 1, buf.at[b], buf.at[SLOTS - d], dn))
        else:
            out.append(remote(n, buf.at[a, 0], buf.at[d, 0], up))
            out.append(remote(n + 1, buf.at[b, 1], buf.at[d, 1], dn))
        return out

    last = NZ // 2
    hops = [None] + [[hop(d, 0), hop(d, 1)] for d in range(1, last + 1)]

    def forward(d, i):
        for copy in hops[d][i]:
            copy.wait_recv()
        if d < last:
            for copy in hops[d + 1][i]:
                copy.start()

    pair = pl.ds(0, 2)
    q_x = [
        remote(QX, qbuf.at[pair], qbuf.at[pl.ds(2, 2)], x_dn),
        remote(QX + 1, qbuf.at[pair], qbuf.at[pl.ds(6, 2)], x_up),
    ]
    q_far = [
        remote(QX + 2, qbuf.at[2], qbuf.at[4], x_dn),
        remote(QX + 3, qbuf.at[7], qbuf.at[5], x_up),
    ]

    wq[...] = jnp.zeros(wq.shape, bf16)
    acc[...] = jnp.zeros(acc.shape, f32)
    lsum[...] = jnp.zeros(lsum.shape, f32)
    tops[...] = jnp.full(tops.shape, NEG, f32)
    k_own.wait()
    v_own.wait()
    k_swap.wait()
    for copy in hops[1][0]:
        copy.start()
    v_swap.wait()
    for copy in hops[1][1]:
        copy.start()
    for copy in w_loads:
        copy.wait()
    for copy in w_first:
        copy.start()

    def body(s_acc, o_acc):
        width = u_ref.shape[1]
        padded[8:] = u_ref[...].astype(f32)
        padded[:8] = jnp.where(sp == 0, 0.0, edge_ref[8:].astype(f32))
        group = lax.broadcasted_iota(jnp.int32, (width, width), 0) // GROUP
        same = group == lax.broadcasted_iota(jnp.int32, (width, width), 1) // GROUP
        mean_of = jnp.where(same, 1.0 / GROUP, 0.0).astype(bf16)

        def conv_block(i, carry):
            at = pl.multiple_of(i * 128, 128)
            window = padded[pl.ds(at, 136)]
            conv = taps_ref[0:1] * window[6:134]
            conv += taps_ref[1:2] * window[7:135]
            conv += taps_ref[2:3] * window[8:136]
            gated = gate_ref[pl.ds(at, 128)].astype(f32) * conv
            square = gated * gated
            high = square.astype(bf16)
            low = (square - high.astype(f32)).astype(bf16)
            pltpu.matmul_push_rhs(mean_of, staging_register=0, mxu_index=0)
            pltpu.matmul_acc_lhs(o_acc[0], high, load_staged_rhs=0)
            pltpu.matmul_acc_lhs(o_acc[0], low)
            mean = pltpu.matmul_pop(o_acc[0])
            conv_loc[i] = (gated * lax.rsqrt(mean + eps) * cgain_ref[...]).astype(bf16)
            return carry

        lax.fori_loop(0, NY, conv_block, 0)

        q_one.wait()

        @pl.when(c == 0)
        def _():
            q_own.wait()

        @pl.when(c == 1)
        def _():
            q_two.wait()

        for copy in q_x:
            copy.start()
        cv_own.start()
        for copy in convs:
            copy.start()

        def prepare(t):
            for m in range(2):
                q = qbuf[t, 64 * m : 64 * m + 64].astype(f32) * LOG2E
                high = q.astype(bf16)
                wq[t, m, 64 * m : 64 * m + 64] = high
                wq[t, m, 128 + 64 * m : 192 + 64 * m] = (q - high.astype(f32)).astype(bf16)

        def q_start(t):
            r, h = t // 2, lax.rem(t, 2)
            zq = jnp.where(h == 0, z, zr)
            return ((zq * NX + wrap(x + r, NX)) * 2 + h) * rows

        def run(t, slots, masked, diff):
            its = [(s, m, g) for m in range(2) for s in slots for g in range(4)]
            n = len(its)
            lag, bufs = 2, 3

            def start(i):
                s, m, g = its[i]
                k = kbuf[s, g // 2, (g % 2) * 256 : (g % 2) * 256 + 256]
                lhs = jnp.concatenate([k, k], axis=1)
                for j in range(2):
                    pltpu.matmul_push_rhs(
                        wq[t, m, :, j * 256 : (j + 1) * 256], staging_register=0, mxu_index=j
                    )
                    pltpu.matmul_acc_lhs(s_acc[j][i % bufs], lhs, load_staged_rhs=0)

            def drain(i, j):
                g = its[i][2]
                sc = pltpu.matmul_pop(s_acc[j][i % bufs])
                if masked:
                    d = lax.broadcasted_iota(jnp.int32, sc.shape, 0) - lax.broadcasted_iota(
                        jnp.int32, sc.shape, 1
                    )
                    sc = jnp.where(d <= diff + (j * 256 - g * 256), sc, NEG)
                return sc

            shift = {}
            if general:
                best = {}
                for i in range(lag):
                    start(i)
                for i in range(n):
                    if i + lag < n:
                        start(i + lag)
                    for j in range(2):
                        top = jnp.max(drain(i, j).reshape(32, 8, 256), axis=0)
                        key = (its[i][1], j)
                        best[key] = jnp.maximum(best[key], top) if key in best else top
                for (m, j), top in best.items():
                    cs = slice(j * 256, (j + 1) * 256)
                    before = tops[t, m : m + 1, cs]
                    now = jnp.maximum(before, jnp.max(top, axis=0, keepdims=True))
                    tops[t, m : m + 1, cs] = now
                    fade = jnp.exp2(before - now)
                    acc[t, m, :, cs] = acc[t, m, :, cs] * fade
                    lsum[t, m, :, cs] = lsum[t, m, :, cs] * fade
                    shift[m, j] = now

            ls = [None, None]
            for i in range(lag):
                start(i)
            for i in range(n):
                s, m, g = its[i]
                if i + lag < n:
                    start(i + lag)
                for j in range(2):
                    sc = drain(i, j)
                    p = jnp.exp2(sc - shift[m, j] if general else sc)
                    one = jnp.sum(p.reshape(32, 8, 256), axis=0)
                    ls[j] = one if ls[j] is None else ls[j] + one
                    pltpu.matmul_push_rhs(p.astype(bf16), staging_register=1, mxu_index=j)
                    pltpu.matmul_acc_lhs(
                        o_acc[j],
                        vbuf[s, g // 2, :, (g % 2) * 256 : (g % 2) * 256 + 256],
                        load_staged_rhs=1,
                    )
                if i + 1 == n or its[i + 1][1] != m:
                    for j in range(2):
                        cs = slice(j * 256, (j + 1) * 256)
                        acc[t, m, :, cs] += pltpu.matmul_pop(o_acc[j])
                        lsum[t, m, :, cs] += ls[j]
                    ls = [None, None]

        def step(u, carry):
            for d in range(1, last + 1):

                @pl.when(u == d)
                def _(d=d):
                    if d > 1:
                        forward(d, 1)
                    if d == 3:
                        for copy in w_first:
                            copy.wait_recv()
                        for copy in w_far + w_core[:2] + w_core[4:]:
                            copy.start()

            sa, sb = u, lax.rem(SLOTS - u, SLOTS)
            two = (u > 0) & (u < last)

            def tile(i, carry):
                t = jnp.where(i < 4, i, jnp.where(i < 6, i + 2, i - 2))

                @pl.when((u == 0) & (i == 0))
                def _():
                    prepare(0)
                    prepare(1)

                @pl.when((u == 0) & (i == 2))
                def _():
                    forward(1, 0)
                    for copy in q_x:
                        copy.wait_recv()
                    for copy in q_far:
                        copy.start()
                    for tt in (2, 3, 6, 7):
                        prepare(tt)

                @pl.when((u == 0) & (i == 6))
                def _():
                    forward(1, 1)
                    for copy in q_far:
                        copy.wait_recv()
                    prepare(4)
                    prepare(5)

                for d in range(2, last + 1):

                    @pl.when((u == d - 1) & (i == 6))
                    def _(d=d):
                        forward(d, 0)

                def diff_of(s):
                    zk = wrap(z - s, NZ)
                    return q_start(t) - (zk * NX + x) * 2 * rows

                da, db = diff_of(sa), diff_of(sb)
                full = 2 * rows
                both = two & (da >= full) & (db >= full)

                @pl.when(both)
                def _():
                    run(t, [sa, sb], False, 0)

                @pl.when(jnp.logical_not(both))
                def _():
                    def one(b, carry):
                        s = jnp.where(b == 0, sa, sb)
                        diff = diff_of(s)

                        @pl.when(diff >= full)
                        def _():
                            run(t, [s], False, 0)

                        @pl.when((diff >= 0) & (diff < full))
                        def _():
                            run(t, [s], True, diff)

                        return carry

                    lax.fori_loop(0, jnp.where(two, 2, 1), one, 0)

                return carry

            lax.fori_loop(0, 2 * NX, tile, 0)
            return carry

        lax.fori_loop(0, last + 1, step, 0)

        for t in range(2 * NX):
            for m in range(2):
                stats[t, m : m + 1] = jnp.sum(lsum[t, m], axis=0, keepdims=True)
            if general:
                stats[t, 2:4] = tops[t]
        st = [
            remote(STAT + r - 1, stats, stats_in.at[r - 1], dev(z, wrap(x - r, NX), c, y))
            for r in range(1, NX)
        ]
        for copy in st:
            copy.start()
        for copy in w_far:
            copy.wait_recv()
        for copy in w_core[2:4]:
            copy.start()
        for copy in st:
            copy.wait_recv()
        lam = lam_ref[c]

        def parts_of(t):
            return [stats[t]] + [stats_in[r - 1, (t - 2 * r) % (2 * NX)] for r in range(1, NX)]

        def total(t):
            each = parts_of(t)
            if not general:
                return each[0] + each[1] + each[2] + each[3], 0.0
            top = functools.reduce(jnp.maximum, [e[2:4] for e in each])
            return sum(e[0:2] * jnp.exp2(e[2:4] - top) for e in each), top

        def partial(t):
            tot, top = total(t)
            own = jnp.exp2(tops[t] - top) if general else jnp.ones_like(tot)
            return acc[t, 0] * (own[0:1] / tot[0:1]) - acc[t, 1] * (lam * own[1:2] / tot[1:2])

        def log_total(t):
            tot, top = total(t)
            return jnp.log(tot) + top * LN2

        part[4] = partial(4).astype(bf16)
        part[5] = partial(5).astype(bf16)
        p_far = [
            remote(PART, part.at[4], part_in.at[0], x_up),
            remote(PART + 1, part.at[5], part_in.at[1], x_dn),
        ]
        for copy in p_far:
            copy.start()
        for t in (2, 3, 6, 7, 0, 1):
            acc[t, 0] = partial(t)
        for h in range(2):
            logs[h] = log_total(h)
        part[3] = acc[3, 0].astype(bf16)
        part[6] = acc[6, 0].astype(bf16)
        for copy in p_far:
            copy.wait_recv()
        part[2] = (acc[2, 0] + part_in[0].astype(f32)).astype(bf16)
        part[7] = (acc[7, 0] + part_in[1].astype(f32)).astype(bf16)
        p_near = [
            remote(PART + 2, part.at[pl.ds(2, 2)], part_in.at[pl.ds(2, 2)], x_up),
            remote(PART + 3, part.at[pl.ds(6, 2)], part_in.at[pl.ds(4, 2)], x_dn),
        ]
        for copy in p_near:
            copy.start()
        for copy in p_near:
            copy.wait_recv()

        gain = jnp.broadcast_to(gain_ref[...], (128, 128)).T
        gain = jnp.concatenate([gain] * NY, axis=1)
        for h in range(2):
            attn = acc[h, 0] + part_in[2 + h].astype(f32) + part_in[4 + h].astype(f32)
            mean = jnp.mean(attn * attn, axis=0, keepdims=True)
            heads_t = (attn * lax.rsqrt(mean + eps) * gain).astype(bf16)
            for yy in range(NY):
                heads[h, yy] = heads_t[:, yy * 128 : (yy + 1) * 128]
        zh = (z, zr)
        own_head = pltpu.make_async_copy(heads.at[0, y], a_in.at[0], local_sem.at[4])
        own_log = pltpu.make_async_copy(logs.at[0], log_out.at[c], local_sem.at[5])
        late = []
        for h in range(2):
            for o in range(NY):
                yy = wrap(y + o, NY)
                copy = pltpu.make_async_remote_copy(
                    src_ref=heads.at[h, yy],
                    dst_ref=a_in.at[2 * o + c],
                    send_sem=s_send.at[HOME + 4 * h + o],
                    recv_sem=s_recv.at[HOME + 2 * o + c],
                    device_id=dev(zh[h], x, h, yy),
                    device_id_type=MESH,
                )
                if h == 0 and o == 0:
                    first = copy
                else:
                    copy.start()
                    late.append(copy)
            copy = pltpu.make_async_remote_copy(
                src_ref=logs.at[h],
                dst_ref=log_out.at[c],
                send_sem=s_send.at[LOGS + h],
                recv_sem=s_recv.at[LOGS + c],
                device_id=dev(zh[h], x, h, y),
                device_id_type=MESH,
            )
            if h == 0:
                first_log = copy
            else:
                copy.start()
                late.append(copy)

        @pl.when(c == 0)
        def _():
            own_head.start()
            own_log.start()

        @pl.when(c == 1)
        def _():
            first.start()
            first_log.start()

        for copy in w_core + convs:
            copy.wait()
        cv_own.wait()

        def product(n, lhs_of, kind):
            out = []
            for j in range(2):
                at = pl.ds(pl.multiple_of((2 * n + j) * 256, 256), 256)
                for d in range(NY):
                    w = w_own[kind, :, at] if d == 0 else w_in[d - 1, kind, :, at]
                    pltpu.matmul_push_rhs(w, staging_register=0, mxu_index=j)
                    pltpu.matmul_acc_lhs(o_acc[j], lhs_of(d), load_staged_rhs=0)
                out.append((at, pltpu.matmul_pop(o_acc[j])))
            return out

        def conv_out_part(n, carry):
            for at, value in product(n, lambda d: cv_in[d], 1):
                out_ref[:, at] = value
            return carry

        lax.fori_loop(0, out_ref.shape[1] // 512, conv_out_part, 0)

        for s in range(2 * NY):

            @pl.when((c == 1) | (s > 0))
            def _(s=s):
                remote(HOME, heads.at[0, 0], a_in.at[s], partner, HOME + s).wait_recv()

        @pl.when(c == 0)
        def _():
            own_head.wait()
            own_log.wait()

        for s in range(2 * NY):
            a_rows[:, s * 128 : (s + 1) * 128] = a_in[s].T

        def head_out_part(n, carry):
            for at, value in product(n, lambda d: a_rows[:, d * 256 : (d + 1) * 256], 0):
                out_ref[:, at] += value
            return carry

        lax.fori_loop(0, out_ref.shape[1] // 512, head_out_part, 0)

        sent = []
        for d in range(1, last + 1):
            sent += hops[d][0] + hops[d][1]
        for copy in sent + q_x + q_far + st + p_far + p_near + late + w_first + w_far:
            copy.wait_send()
        for s in range(2):

            @pl.when((c == 1) | (s == 1))
            def _(s=s):
                remote(LOGS, logs.at[0], log_out.at[s], partner, LOGS + s).wait_recv()

        @pl.when(c == 1)
        def _():
            first.wait_send()
            first_log.wait_send()

    def made(q, count):
        return pltpu.ACC(q)((count, 256), f32)

    pl.run_scoped(
        body, [[made(q, 256) for _ in range(3)] for q in range(2)], [made(q, 128) for q in range(2)]
    )


def fused(
    general, kn, value_t, qn_t, u, gate, edge, taps, cgain, w_att, w_conv, lambdas, sub_gain
):
    f32, bf16 = jnp.float32, jnp.bfloat16
    rows = kn.shape[1]
    own, channels, width = rows // NY, u.shape[1], w_att.shape[1]
    vm = pl.BlockSpec(memory_space=pltpu.VMEM)
    hbm = pl.BlockSpec(memory_space=pltpu.HBM)
    sm = pl.BlockSpec(memory_space=pltpu.SMEM)
    tiles = 2 * NX
    return pl.pallas_call(
        functools.partial(fused_kernel, general),
        in_specs=[vm] * 8 + [hbm, hbm, sm, vm],
        out_specs=[vm, vm],
        out_shape=[
            jax.ShapeDtypeStruct((own, width), f32),
            jax.ShapeDtypeStruct((2, 2, rows), f32),
        ],
        scratch_shapes=[
            pltpu.VMEM((SLOTS, 2, rows, 128), bf16),
            pltpu.VMEM((SLOTS, 2, 128, rows), bf16),
            pltpu.VMEM((tiles, 128, rows), bf16),
            pltpu.VMEM((tiles, 2, 256, rows), bf16),
            pltpu.VMEM((tiles, 2, 128, rows), f32),
            pltpu.VMEM((tiles, 2, 8, rows), f32),
            pltpu.VMEM((tiles, 4 if general else 2, rows), f32),
            pltpu.VMEM((NX - 1, tiles, 4 if general else 2, rows), f32),
            pltpu.VMEM((tiles, 128, rows), bf16),
            pltpu.VMEM((6, 128, rows), bf16),
            pltpu.VMEM((2, NY, 128, 128), bf16),
            pltpu.VMEM((2, 2, rows), f32),
            pltpu.VMEM((NY, own, channels), bf16),
            pltpu.VMEM((2 * NY, 128, 128), bf16),
            pltpu.VMEM((NY, own, channels), bf16),
            pltpu.VMEM((2, *w_att.shape), bf16),
            pltpu.VMEM((NY - 1, 2, *w_att.shape), bf16),
            pltpu.VMEM((rows + 8, channels), f32),
            pltpu.VMEM((own, NY * 256), bf16),
            pltpu.VMEM((tiles, 2, rows), f32),
            pltpu.SemaphoreType.DMA((56,)),
            pltpu.SemaphoreType.DMA((56,)),
            pltpu.SemaphoreType.DMA((8,)),
        ],
        cost_estimate=pl.CostEstimate(
            flops=2 * 10**10, bytes_accessed=16 * 2**20, transcendentals=34 * 10**6
        ),
        compiler_params=pltpu.CompilerParams(
            collective_id=2 if general else 1, has_side_effects=True, vmem_limit_bytes=63 * 1024 * 1024
        ),
    )(kn, value_t, qn_t, u, gate, edge, taps, cgain, w_att, w_conv, lambdas, sub_gain)


def on_device(
    inputs,
    norm_gain,
    w_query,
    w_key,
    w_value,
    query_gain,
    key_gain,
    lambdas,
    sub_gain,
    w_gate_b,
    w_gate_c,
    w_conv_in,
    conv_taps,
    conv_gain,
    w_out_att,
    w_out_conv,
):
    comp = query_gain.shape[1]
    made = front(
        inputs,
        norm_gain[None],
        query_gain,
        key_gain,
        w_query,
        w_key,
        w_value,
        w_gate_b,
        w_gate_c,
        w_conv_in,
    )
    reach = jnp.max(jnp.abs(query_gain * key_gain)) * (comp**0.5) * LOG2E * 1.02
    return tuple(
        lax.cond(
            reach < 90.0,
            functools.partial(fused, False),
            functools.partial(fused, True),
            *made,
            conv_taps,
            conv_gain[None],
            w_out_att,
            w_out_conv,
            lambdas,
            sub_gain[None],
        )
    )


def solution(mesh):
    in_specs = (
        P(("sp", "tp"), None),
        P(),
        P(None, "tp"),
        P(None, "tp"),
        P(None, "tp"),
        P(),
        P(),
        P("tp"),
        P(),
        P(None, "tp"),
        P(None, "tp"),
        P(None, "tp"),
        P(None, "tp"),
        P("tp"),
        P("tp", None),
        P("tp", None),
    )
    out_specs = (P(("sp", "tp"), None), P("tp", None, "sp"))
    return jax.shard_map(
        on_device, mesh=mesh, in_specs=in_specs, out_specs=out_specs, check_vma=False
    )
```

```python
import functools

import jax
import jax.numpy as jnp
from jax import lax
from jax.experimental import pallas as pl
from jax.experimental.pallas import tpu as pltpu
from jax.sharding import PartitionSpec as P

NZ, NX, NY = 8, 4, 4
GROUP = 64
LOG2E = 1.4426950408889634
LN2 = 0.6931471805599453
NEG = -1e30
eps = 1e-06


MESH = pl.DeviceIdType.MESH
SLOTS = 8


def fused_kernel(
    general,
    x_ref,
    ngain_ref,
    qgain_ref,
    kgain_ref,
    wq_ref,
    wk_ref,
    wv_ref,
    wb_ref,
    wc_ref,
    wi_ref,
    taps_ref,
    cgain_ref,
    w_att,
    w_conv,
    lam_ref,
    gain_ref,
    out_ref,
    log_out,
    xbuf,
    weights,
    gains,
    k_loc,
    v_loc,
    q_loc,
    u_loc,
    gate_loc,
    edge_buf,
    kbuf,
    vbuf,
    qbuf,
    wq,
    acc,
    lsum,
    stats,
    stats_in,
    part,
    part_in,
    heads,
    logs,
    conv_loc,
    a_in,
    cv_in,
    w_own,
    w_in,
    padded,
    a_rows,
    tops,
    s_send,
    s_recv,
    local_sem,
):
    f32, bf16 = jnp.float32, jnp.bfloat16
    sp = lax.axis_index("sp")
    y = lax.axis_index("tp")
    z = sp // (2 * NX)
    x = lax.rem(sp // 2, NX)
    c = lax.rem(sp, 2)
    zr = NZ - 1 - z
    rows = 512

    def dev(zz, xx, cc, yy):
        return ((zz * NX + xx) * 2 + cc, yy)

    def wrap(v, n):
        return lax.rem(v + n, n)

    z_up, z_dn = wrap(z + 1, NZ), wrap(z - 1, NZ)
    x_up, x_dn = dev(z, wrap(x + 1, NX), c, y), dev(z, wrap(x - 1, NX), c, y)
    up, dn = wrap(y + 1, NY), wrap(y - 1, NY)
    y_up, y_dn = dev(z, x, c, up), dev(z, x, c, dn)
    partner = dev(z, x, 1 - c, y)
    after, before = wrap(sp + 1, NZ * NX * 2), wrap(sp - 1, NZ * NX * 2)

    p_loads = [
        pltpu.make_async_copy(ref, weights.at[i], local_sem.at[i])
        for i, ref in enumerate((wk_ref, wv_ref, wq_ref, wc_ref, wi_ref, wb_ref))
    ]
    for copy in p_loads:
        copy.start()
    w_loads = [
        pltpu.make_async_copy(w_att, w_own.at[0], local_sem.at[6]),
        pltpu.make_async_copy(w_conv, w_own.at[1], local_sem.at[7]),
    ]
    for copy in w_loads:
        copy.start()

    barrier = pltpu.get_barrier_semaphore()
    peers = [dev(zz, x, cc, y) for zz in (z_up, z_dn) for cc in (c, 1 - c)]
    peers += [(after, y), (before, y)]
    peers += [dev(z, wrap(x + r, NX), c, y) for r in range(1, NX)]
    for o in range(NY):
        yy = wrap(y + o, NY)
        if o:
            peers.append(dev(z, x, c, yy))
        peers.append(dev(z, x, 1 - c, yy))
        peers.append(dev(zr, x, c, yy))
        peers.append(dev(zr, x, 1 - c, yy))
    for peer in peers:
        pl.semaphore_signal(barrier, inc=1, device_id=peer, device_id_type=MESH)

    own = x_ref.shape[0]
    piece = 16

    def norm(i, carry):
        at = pl.ds(pl.multiple_of(i * piece, piece), piece)
        v = x_ref[at].astype(f32)
        scale = lax.rsqrt(jnp.mean(v * v, axis=1, keepdims=True) + eps)
        xbuf[y, at] = (v * scale * ngain_ref[...]).astype(bf16)
        return carry

    lax.fori_loop(0, own // piece, norm, 0)
    for i, (ref, scale) in enumerate(((qgain_ref, 0.125), (kgain_ref, 1.0))):
        row = jnp.concatenate([ref[0:1], ref[1:2]], axis=1) * scale
        gains[i] = jnp.broadcast_to(row, (128, 128)).T
    pl.semaphore_wait(barrier, len(peers))

    numbers = [0]

    def new(count=1):
        numbers[0] += count
        return numbers[0] - count

    def remote(n, src, dst, to, m=None):
        return pltpu.make_async_remote_copy(
            src_ref=src,
            dst_ref=dst,
            send_sem=s_send.at[n],
            recv_sem=s_recv.at[n if m is None else m],
            device_id=to,
            device_id_type=MESH,
        )

    STAT, PART, HOME, LOGS, CONV, WY, WF, WC = (
        new(3), new(4), new(8), new(2), new(3), new(4), new(2), new(6)
    )

    half = own // 2

    def x_part(s, h):
        return xbuf.at[s, pl.ds(h * half, half)]

    x_one = [
        remote(new(), x_part(y, 0), x_part(y, 0), y_up),
        remote(new(), x_part(y, 1), x_part(y, 1), y_dn),
        remote(new(), x_part(y, 1), x_part(y, 1), y_up),
        remote(new(), x_part(y, 0), x_part(y, 0), y_dn),
    ]
    for copy in x_one:
        copy.start()
    x_far = [
        remote(new(), x_part(dn, 0), x_part(dn, 0), y_up),
        remote(new(), x_part(up, 1), x_part(up, 1), y_dn),
    ]
    edge = remote(new(), u_loc.at[pl.ds(rows - 16, 16)], edge_buf, (after, y))

    slots_y = [y, dn, up, wrap(y + 2, NY)]
    last = NZ // 2
    both_cores = pl.ds(0, 2)

    def k_at(slot, core, s):
        return kbuf.at[slot, core, pl.ds(pl.multiple_of(s * 128, 128), 128)]

    def v_at(slot, core, s):
        return vbuf.at[slot, core, s]

    at_of = (k_at, v_at)
    swaps, hop_one, hop_in, hops, q_one, q_two, q_x, q_far = [], [], [], {}, [], [], [], []
    q_to = dev(jnp.where(c == 0, z, zr), x, 1 - c, y)
    for i, s in enumerate(slots_y):
        swap, sends, waits = [], [], []
        for kv in range(2):
            if kv == 0:
                src = [k_loc.at[h, pl.ds(pl.multiple_of(s * 128, 128), 128)] for h in range(2)]
                other = k_loc.at[1 - c, pl.ds(pl.multiple_of(s * 128, 128), 128)]
            else:
                src = [v_loc.at[h, s] for h in range(2)]
                other = v_loc.at[1 - c, s]
            swap.append(remote(new(), other, at_of[kv](0, c, s), partner))
            for zz, slot in ((z_up, 1), (z_dn, SLOTS - 1)):
                n = new(2)
                for h in range(2):
                    sends.append(
                        remote(n + h, src[h], at_of[kv](slot, c, s), dev(zz, x, h, y), n + c)
                    )
                    waits.append(
                        remote(n + h, src[h], at_of[kv](slot, h, s), partner, n + h)
                    )
            for d in range(2, last + 1):
                for zz, a, b, core in (
                    (z_up, d - 1, d, 0),
                    (z_dn, SLOTS - d + 1, SLOTS - d, 1),
                ):
                    pick = both_cores if d < last else core
                    hops.setdefault((d, i), []).append(
                        remote(new(), at_of[kv](a, pick, s), at_of[kv](b, pick, s), dev(zz, x, c, y))
                    )
        swaps.append(swap)
        hop_one.append(sends)
        hop_in.append(waits)
        q_one.append(remote(new(), q_loc.at[1 - c, s], qbuf.at[c, s], q_to))
        q_two.append(remote(new(), q_loc.at[1, s], qbuf.at[1, s], dev(zr, x, 1, y)))
        pair = pl.ds(0, 2)
        q_x.append(
            [
                remote(new(), qbuf.at[pair, s], qbuf.at[pl.ds(2, 2), s], x_dn),
                remote(new(), qbuf.at[pair, s], qbuf.at[pl.ds(6, 2), s], x_up),
            ]
        )
        q_far.append(
            [
                remote(new(), qbuf.at[2, s], qbuf.at[4, s], x_dn),
                remote(new(), qbuf.at[7, s], qbuf.at[5, s], x_up),
            ]
        )
    assert numbers[0] <= s_send.shape[0]

    def w_half(kind, cc):
        return w_own.at[kind, pl.ds(cc * 128, 128)]

    def w_slot(d, kind, cc):
        return w_in.at[d - 1, kind, pl.ds(cc * 128, 128)]

    w_first = [
        remote(WY, w_half(0, c), w_slot(1, 0, c), y_up),
        remote(WY + 1, w_half(1, c), w_slot(1, 1, c), y_up),
        remote(WY + 2, w_half(0, c), w_slot(3, 0, c), y_dn),
        remote(WY + 3, w_half(1, c), w_slot(3, 1, c), y_dn),
    ]
    w_far = [
        remote(WF, w_slot(1, 0, c), w_slot(2, 0, c), y_up),
        remote(WF + 1, w_slot(3, 1, c), w_slot(2, 1, c), y_dn),
    ]
    w_core = [
        remote(WC + 2 * (d - 1) + kind, w_slot(d, kind, c), w_slot(d, kind, c), partner)
        for d in range(1, NY)
        for kind in range(2)
    ]
    convs = [
        remote(
            CONV + o - 1,
            conv_loc.at[wrap(y + o, NY)],
            cv_in.at[o],
            dev(z, x, c, wrap(y + o, NY)),
        )
        for o in range(1, NY)
    ]
    cv_own = pltpu.make_async_copy(conv_loc.at[y], cv_in.at[0], local_sem.at[3])

    def body(s_acc, o_acc):
        def project(s):
            at = pl.ds(pl.multiple_of(s * own, own), own)
            out = []
            for n in range(6):
                j = n % 2
                for t in range(8):
                    pltpu.matmul_push_rhs(
                        weights[n, t * 256 : (t + 1) * 256], staging_register=0, mxu_index=j
                    )
                    pltpu.matmul_acc_lhs(
                        o_acc[j], xbuf[s, :, t * 256 : (t + 1) * 256], load_staged_rhs=0
                    )
                out.append(pltpu.matmul_pop(o_acc[j]).astype(bf16).astype(f32))

            def scaled(v):
                r = v.T.reshape(4, 64, own)
                r = r * lax.rsqrt(jnp.mean(r * r, axis=1, keepdims=True) + eps)
                return r.reshape(2, 128, own)

            k = scaled(out[0])
            k = [(k[h] * gains[1]).T.astype(bf16) for h in range(2)]
            v = out[1].T.astype(bf16)
            v = [v[:128], v[128:]]
            q = scaled(out[2])
            for h in range(2):
                k_loc[h, at] = k[h]
                v_loc[h, s] = v[h]
                q_loc[h, s] = (q[h] * gains[0]).astype(bf16)

                @pl.when(c == h)
                def _(h=h):
                    kbuf[0, h, at] = k[h]
                    vbuf[0, h, s] = v[h]

            @pl.when(c == 0)
            def _():
                qbuf[0, s] = (q[0] * gains[0]).astype(bf16)

            u_loc[at] = (out[3] * out[4]).astype(bf16)
            gate_loc[at] = out[5].astype(bf16)

            @pl.when(s == NY - 1)
            def _():
                edge.start()

        def launch(i):
            for copy in hop_one[i] + swaps[i]:
                copy.start()
            q_one[i].start()

            @pl.when(c == 1)
            def _():
                q_two[i].start()

        def second(i):
            q_one[i].wait_recv()

            @pl.when(c == 1)
            def _():
                q_two[i].wait_recv()

            for copy in q_x[i]:
                copy.start()
            for copy in hop_in[i]:
                copy.wait_recv()
            for copy in hops[2, i]:
                copy.start()

        def third(i):
            for copy in q_x[i]:
                copy.wait_recv()
            for copy in q_far[i]:
                copy.start()
            for copy in hops[2, i]:
                copy.wait_recv()
            for copy in hops[3, i]:
                copy.start()

        def fourth(i):
            for copy in hops[3, i]:
                copy.wait_recv()
            for copy in hops[4, i]:
                copy.start()

        for copy in p_loads:
            copy.wait()
        project(slots_y[0])
        launch(0)
        x_one[0].wait_recv()
        x_far[0].start()
        x_one[1].wait_recv()
        x_far[1].start()
        second(0)
        wq[...] = jnp.zeros(wq.shape, bf16)
        acc[...] = jnp.zeros(acc.shape, f32)
        lsum[...] = jnp.zeros(lsum.shape, f32)
        tops[...] = jnp.full(tops.shape, NEG, f32)
        x_one[2].wait_recv()
        project(slots_y[1])
        launch(1)
        x_one[3].wait_recv()
        project(slots_y[2])
        launch(2)
        third(0)
        second(1)
        for copy in x_far:
            copy.wait_recv()
        project(slots_y[3])
        launch(3)
        for copy in w_loads:
            copy.wait()
        for copy in w_first:
            copy.start()
        second(2)
        fourth(0)
        third(1)

        edge.wait_recv()
        width = u_loc.shape[1]
        padded[8:] = u_loc[...].astype(f32)
        padded[:8] = jnp.where(sp == 0, 0.0, edge_buf[8:].astype(f32))
        group = lax.broadcasted_iota(jnp.int32, (width, width), 0) // GROUP
        same = group == lax.broadcasted_iota(jnp.int32, (width, width), 1) // GROUP
        mean_of = jnp.where(same, 1.0 / GROUP, 0.0).astype(bf16)

        def conv_block(i, carry):
            at = pl.multiple_of(i * 128, 128)
            window = padded[pl.ds(at, 136)]
            conv = taps_ref[0:1] * window[6:134]
            conv += taps_ref[1:2] * window[7:135]
            conv += taps_ref[2:3] * window[8:136]
            gated = gate_loc[pl.ds(at, 128)].astype(f32) * conv
            square = gated * gated
            high = square.astype(bf16)
            low = (square - high.astype(f32)).astype(bf16)
            pltpu.matmul_push_rhs(mean_of, staging_register=0, mxu_index=0)
            pltpu.matmul_acc_lhs(o_acc[0], high, load_staged_rhs=0)
            pltpu.matmul_acc_lhs(o_acc[0], low)
            mean = pltpu.matmul_pop(o_acc[0])
            conv_loc[i] = (gated * lax.rsqrt(mean + eps) * cgain_ref[...]).astype(bf16)
            return carry

        lax.fori_loop(0, NY, conv_block, 0)
        cv_own.start()
        for copy in convs:
            copy.start()
        second(3)
        third(2)

        def prepare(t):
            for s in range(NY):
                cs = slice(s * 128, (s + 1) * 128)
                for m in range(2):
                    q = qbuf[t, s, 64 * m : 64 * m + 64].astype(f32) * LOG2E
                    high = q.astype(bf16)
                    wq[t, m, 64 * m : 64 * m + 64, cs] = high
                    wq[t, m, 128 + 64 * m : 192 + 64 * m, cs] = (q - high.astype(f32)).astype(bf16)

        def prepare_all(lo, hi):
            def each(i, carry):
                prepare(i)
                return carry

            lax.fori_loop(lo, hi, each, 0)

        for swap in swaps:
            for copy in swap:
                copy.wait_recv()

        def q_start(t):
            r, h = t // 2, lax.rem(t, 2)
            zq = jnp.where(h == 0, z, zr)
            return ((zq * NX + wrap(x + r, NX)) * 2 + h) * rows

        def v_chunk(s, g):
            a = 2 * (g % 2)
            return jnp.concatenate([vbuf[s, g // 2, a], vbuf[s, g // 2, a + 1]], axis=1)

        def run(t, slots, masked, diff):
            its = [(s, m, g) for m in range(2) for s in slots for g in range(4)]
            n = len(its)
            lag, bufs = 2, 3

            def start(i):
                s, m, g = its[i]
                k = kbuf[s, g // 2, (g % 2) * 256 : (g % 2) * 256 + 256]
                lhs = jnp.concatenate([k, k], axis=1)
                for j in range(2):
                    pltpu.matmul_push_rhs(
                        wq[t, m, :, j * 256 : (j + 1) * 256], staging_register=0, mxu_index=j
                    )
                    pltpu.matmul_acc_lhs(s_acc[j][i % bufs], lhs, load_staged_rhs=0)

            def drain(i, j):
                g = its[i][2]
                sc = pltpu.matmul_pop(s_acc[j][i % bufs])
                if masked:
                    d = lax.broadcasted_iota(jnp.int32, sc.shape, 0) - lax.broadcasted_iota(
                        jnp.int32, sc.shape, 1
                    )
                    sc = jnp.where(d <= diff + (j * 256 - g * 256), sc, NEG)
                return sc

            shift = {}
            if general:
                best = {}
                for i in range(lag):
                    start(i)
                for i in range(n):
                    if i + lag < n:
                        start(i + lag)
                    for j in range(2):
                        top = jnp.max(drain(i, j).reshape(32, 8, 256), axis=0)
                        key = (its[i][1], j)
                        best[key] = jnp.maximum(best[key], top) if key in best else top
                for (m, j), top in best.items():
                    cs = slice(j * 256, (j + 1) * 256)
                    before = tops[t, m : m + 1, cs]
                    now = jnp.maximum(before, jnp.max(top, axis=0, keepdims=True))
                    tops[t, m : m + 1, cs] = now
                    fade = jnp.exp2(before - now)
                    acc[t, m, :, cs] = acc[t, m, :, cs] * fade
                    lsum[t, m, :, cs] = lsum[t, m, :, cs] * fade
                    shift[m, j] = now

            ls = [None, None]
            for i in range(lag):
                start(i)
            for i in range(n):
                s, m, g = its[i]
                if i + lag < n:
                    start(i + lag)
                for j in range(2):
                    sc = drain(i, j)
                    p = jnp.exp2(sc - shift[m, j] if general else sc)
                    one = jnp.sum(p.reshape(32, 8, 256), axis=0)
                    ls[j] = one if ls[j] is None else ls[j] + one
                    pltpu.matmul_push_rhs(p.astype(bf16), staging_register=1, mxu_index=j)
                    pltpu.matmul_acc_lhs(
                        o_acc[j],
                        v_chunk(s, g),
                        load_staged_rhs=1,
                    )
                if i + 1 == n or its[i + 1][1] != m:
                    for j in range(2):
                        cs = slice(j * 256, (j + 1) * 256)
                        acc[t, m, :, cs] += pltpu.matmul_pop(o_acc[j])
                        lsum[t, m, :, cs] += ls[j]
                    ls = [None, None]

        def step(u, carry):
            @pl.when(u == 3)
            def _():
                for copy in w_first:
                    copy.wait_recv()
                for copy in w_far + w_core[:2] + w_core[4:]:
                    copy.start()

            @pl.when(u == last)
            def _():
                for i in range(NY):
                    for copy in hops[last, i]:
                        copy.wait_recv()

            sa, sb = u, lax.rem(SLOTS - u, SLOTS)
            two = (u > 0) & (u < last)

            def tile(i, carry):
                t = jnp.where(i < 4, i, jnp.where(i < 6, i + 2, i - 2))

                @pl.when((u == 0) & (i == 0))
                def _():
                    prepare_all(0, 2)

                @pl.when((u == 0) & (i == 2))
                def _():
                    third(3)
                    prepare_all(2, 4)
                    prepare_all(6, 8)

                @pl.when((u == 0) & (i == 6))
                def _():
                    for copies in q_far:
                        for copy in copies:
                            copy.wait_recv()
                    prepare_all(4, 6)
                    fourth(1)

                @pl.when((u == 1) & (i == 0))
                def _():
                    fourth(2)

                @pl.when((u == 1) & (i == 3))
                def _():
                    fourth(3)

                def diff_of(s):
                    zk = wrap(z - s, NZ)
                    return q_start(t) - (zk * NX + x) * 2 * rows

                da, db = diff_of(sa), diff_of(sb)
                full = 2 * rows
                both = two & (da >= full) & (db >= full)

                @pl.when(both)
                def _():
                    run(t, [sa, sb], False, 0)

                @pl.when(jnp.logical_not(both))
                def _():
                    def one(b, carry):
                        s = jnp.where(b == 0, sa, sb)
                        diff = diff_of(s)

                        @pl.when(diff >= full)
                        def _():
                            run(t, [s], False, 0)

                        @pl.when((diff >= 0) & (diff < full))
                        def _():
                            run(t, [s], True, diff)

                        return carry

                    lax.fori_loop(0, jnp.where(two, 2, 1), one, 0)

                return carry

            lax.fori_loop(0, 2 * NX, tile, 0)
            return carry

        lax.fori_loop(0, last + 1, step, 0)

        for t in range(2 * NX):
            for m in range(2):
                stats[t, m : m + 1] = jnp.sum(lsum[t, m], axis=0, keepdims=True)
            if general:
                stats[t, 2:4] = tops[t]
        st = [
            remote(STAT + r - 1, stats, stats_in.at[r - 1], dev(z, wrap(x - r, NX), c, y))
            for r in range(1, NX)
        ]
        for copy in st:
            copy.start()
        for copy in st:
            copy.wait_recv()
        lam = lam_ref[c]

        def parts_of(t):
            return [stats[t]] + [stats_in[r - 1, (t - 2 * r) % (2 * NX)] for r in range(1, NX)]

        def total(t):
            each = parts_of(t)
            if not general:
                return each[0] + each[1] + each[2] + each[3], 0.0
            top = functools.reduce(jnp.maximum, [e[2:4] for e in each])
            return sum(e[0:2] * jnp.exp2(e[2:4] - top) for e in each), top

        def partial(t):
            tot, top = total(t)
            own = jnp.exp2(tops[t] - top) if general else jnp.ones_like(tot)
            return acc[t, 0] * (own[0:1] / tot[0:1]) - acc[t, 1] * (lam * own[1:2] / tot[1:2])

        def log_total(t):
            tot, top = total(t)
            return jnp.log(tot) + top * LN2

        part[4] = partial(4).astype(bf16)
        part[5] = partial(5).astype(bf16)
        p_far = [
            remote(PART, part.at[4], part_in.at[0], x_up),
            remote(PART + 1, part.at[5], part_in.at[1], x_dn),
        ]
        for copy in p_far:
            copy.start()
        for t in (2, 3, 6, 7, 0, 1):
            acc[t, 0] = partial(t)
        for h in range(2):
            logs[h] = log_total(h)
        part[3] = acc[3, 0].astype(bf16)
        part[6] = acc[6, 0].astype(bf16)
        for copy in w_far:
            copy.wait_recv()
        for copy in w_core[2:4]:
            copy.start()
        for copy in p_far:
            copy.wait_recv()
        part[2] = (acc[2, 0] + part_in[0].astype(f32)).astype(bf16)
        part[7] = (acc[7, 0] + part_in[1].astype(f32)).astype(bf16)
        p_near = [
            remote(PART + 2, part.at[pl.ds(2, 2)], part_in.at[pl.ds(2, 2)], x_up),
            remote(PART + 3, part.at[pl.ds(6, 2)], part_in.at[pl.ds(4, 2)], x_dn),
        ]
        for copy in p_near:
            copy.start()
        for copy in p_near:
            copy.wait_recv()

        gain = jnp.broadcast_to(gain_ref[...], (128, 128)).T
        gain = jnp.concatenate([gain] * NY, axis=1)
        for h in range(2):
            attn = acc[h, 0] + part_in[2 + h].astype(f32) + part_in[4 + h].astype(f32)
            mean = jnp.mean(attn * attn, axis=0, keepdims=True)
            heads_t = (attn * lax.rsqrt(mean + eps) * gain).astype(bf16)
            for yy in range(NY):
                heads[h, yy] = heads_t[:, yy * 128 : (yy + 1) * 128]
        zh = (z, zr)
        own_head = pltpu.make_async_copy(heads.at[0, y], a_in.at[0], local_sem.at[4])
        own_log = pltpu.make_async_copy(logs.at[0], log_out.at[c], local_sem.at[5])
        late = []
        for h in range(2):
            for o in range(NY):
                yy = wrap(y + o, NY)
                copy = pltpu.make_async_remote_copy(
                    src_ref=heads.at[h, yy],
                    dst_ref=a_in.at[2 * o + c],
                    send_sem=s_send.at[HOME + 4 * h + o],
                    recv_sem=s_recv.at[HOME + 2 * o + c],
                    device_id=dev(zh[h], x, h, yy),
                    device_id_type=MESH,
                )
                if h == 0 and o == 0:
                    first = copy
                else:
                    copy.start()
                    late.append(copy)
            copy = pltpu.make_async_remote_copy(
                src_ref=logs.at[h],
                dst_ref=log_out.at[c],
                send_sem=s_send.at[LOGS + h],
                recv_sem=s_recv.at[LOGS + c],
                device_id=dev(zh[h], x, h, y),
                device_id_type=MESH,
            )
            if h == 0:
                first_log = copy
            else:
                copy.start()
                late.append(copy)

        @pl.when(c == 0)
        def _():
            own_head.start()
            own_log.start()

        @pl.when(c == 1)
        def _():
            first.start()
            first_log.start()

        for copy in w_core + convs:
            copy.wait()
        cv_own.wait()

        def product(n, lhs_of, kind):
            out = []
            for j in range(2):
                at = pl.ds(pl.multiple_of((2 * n + j) * 256, 256), 256)
                for d in range(NY):
                    w = w_own[kind, :, at] if d == 0 else w_in[d - 1, kind, :, at]
                    pltpu.matmul_push_rhs(w, staging_register=0, mxu_index=j)
                    pltpu.matmul_acc_lhs(o_acc[j], lhs_of(d), load_staged_rhs=0)
                out.append((at, pltpu.matmul_pop(o_acc[j])))
            return out

        def conv_out_part(n, carry):
            for at, value in product(n, lambda d: cv_in[d], 1):
                out_ref[:, at] = value
            return carry

        lax.fori_loop(0, out_ref.shape[1] // 512, conv_out_part, 0)

        for s in range(2 * NY):

            @pl.when((c == 1) | (s > 0))
            def _(s=s):
                remote(HOME, heads.at[0, 0], a_in.at[s], partner, HOME + s).wait_recv()

        @pl.when(c == 0)
        def _():
            own_head.wait()
            own_log.wait()

        for s in range(2 * NY):
            a_rows[:, s * 128 : (s + 1) * 128] = a_in[s].T

        def head_out_part(n, carry):
            for at, value in product(n, lambda d: a_rows[:, d * 256 : (d + 1) * 256], 0):
                out_ref[:, at] += value
            return carry

        lax.fori_loop(0, out_ref.shape[1] // 512, head_out_part, 0)

        sent = x_one + x_far + [edge] + st + p_far + p_near + late + w_first + w_far + q_one
        for i in range(NY):
            sent += swaps[i] + hop_one[i] + q_x[i] + q_far[i]
            for d in range(2, last + 1):
                sent += hops[d, i]
        for copy in sent:
            copy.wait_send()

        @pl.when(c == 1)
        def _():
            for copy in q_two:
                copy.wait_send()

        for s in range(2):

            @pl.when((c == 1) | (s == 1))
            def _(s=s):
                remote(LOGS, logs.at[0], log_out.at[s], partner, LOGS + s).wait_recv()

        @pl.when(c == 1)
        def _():
            first.wait_send()
            first_log.wait_send()

    def made(q, count):
        return pltpu.ACC(q)((count, 256), f32)

    pl.run_scoped(
        body, [[made(q, 256) for _ in range(3)] for q in range(2)], [made(q, 128) for q in range(2)]
    )


def fused(general, inputs, *others):
    f32, bf16 = jnp.float32, jnp.bfloat16
    own, model = inputs.shape
    w_att = others[11]
    rows, channels, width = own * NY, w_att.shape[0], w_att.shape[1]
    vm = pl.BlockSpec(memory_space=pltpu.VMEM)
    hbm = pl.BlockSpec(memory_space=pltpu.HBM)
    sm = pl.BlockSpec(memory_space=pltpu.SMEM)
    tiles = 2 * NX
    count = 160
    return pl.pallas_call(
        functools.partial(fused_kernel, general),
        in_specs=[vm] * 4 + [hbm] * 6 + [vm, vm, hbm, hbm, sm, vm],
        out_specs=[vm, vm],
        out_shape=[
            jax.ShapeDtypeStruct((own, width), f32),
            jax.ShapeDtypeStruct((2, 2, rows), f32),
        ],
        scratch_shapes=[
            pltpu.VMEM((NY, own, model), bf16),
            pltpu.VMEM((6, model, channels), bf16),
            pltpu.VMEM((2, 128, 128), f32),
            pltpu.VMEM((2, rows, 128), bf16),
            pltpu.VMEM((2, NY, 128, 128), bf16),
            pltpu.VMEM((2, NY, 128, 128), bf16),
            pltpu.VMEM((rows, channels), bf16),
            pltpu.VMEM((rows, channels), bf16),
            pltpu.VMEM((16, channels), bf16),
            pltpu.VMEM((SLOTS, 2, rows, 128), bf16),
            pltpu.VMEM((SLOTS, 2, NY, 128, 128), bf16),
            pltpu.VMEM((tiles, NY, 128, 128), bf16),
            pltpu.VMEM((tiles, 2, 256, rows), bf16),
            pltpu.VMEM((tiles, 2, 128, rows), f32),
            pltpu.VMEM((tiles, 2, 8, rows), f32),
            pltpu.VMEM((tiles, 4 if general else 2, rows), f32),
            pltpu.VMEM((NX - 1, tiles, 4 if general else 2, rows), f32),
            pltpu.VMEM((tiles, 128, rows), bf16),
            pltpu.VMEM((6, 128, rows), bf16),
            pltpu.VMEM((2, NY, 128, 128), bf16),
            pltpu.VMEM((2, 2, rows), f32),
            pltpu.VMEM((NY, own, channels), bf16),
            pltpu.VMEM((2 * NY, 128, 128), bf16),
            pltpu.VMEM((NY, own, channels), bf16),
            pltpu.VMEM((2, *w_att.shape), bf16),
            pltpu.VMEM((NY - 1, 2, *w_att.shape), bf16),
            pltpu.VMEM((rows + 8, channels), f32),
            pltpu.VMEM((own, NY * 256), bf16),
            pltpu.VMEM((tiles, 2, rows), f32),
            pltpu.SemaphoreType.DMA((count,)),
            pltpu.SemaphoreType.DMA((count,)),
            pltpu.SemaphoreType.DMA((8,)),
        ],
        cost_estimate=pl.CostEstimate(
            flops=2 * 10**10, bytes_accessed=16 * 2**20, transcendentals=34 * 10**6
        ),
        compiler_params=pltpu.CompilerParams(
            collective_id=1 if general else 0,
            has_side_effects=True,
            vmem_limit_bytes=63 * 1024 * 1024,
        ),
    )(inputs, *others)


def on_device(
    inputs,
    norm_gain,
    w_query,
    w_key,
    w_value,
    query_gain,
    key_gain,
    lambdas,
    sub_gain,
    w_gate_b,
    w_gate_c,
    w_conv_in,
    conv_taps,
    conv_gain,
    w_out_att,
    w_out_conv,
):
    comp = query_gain.shape[1]
    reach = jnp.max(jnp.abs(query_gain * key_gain)) * (comp**0.5) * LOG2E * 1.02
    return tuple(
        lax.cond(
            reach < 90.0,
            functools.partial(fused, False),
            functools.partial(fused, True),
            inputs,
            norm_gain[None],
            query_gain,
            key_gain,
            w_query,
            w_key,
            w_value,
            w_gate_b,
            w_gate_c,
            w_conv_in,
            conv_taps,
            conv_gain[None],
            w_out_att,
            w_out_conv,
            lambdas,
            sub_gain[None],
        )
    )


def solution(mesh):
    in_specs = (
        P(("sp", "tp"), None),
        P(),
        P(None, "tp"),
        P(None, "tp"),
        P(None, "tp"),
        P(),
        P(),
        P("tp"),
        P(),
        P(None, "tp"),
        P(None, "tp"),
        P(None, "tp"),
        P(None, "tp"),
        P("tp"),
        P("tp", None),
        P("tp", None),
    )
    out_specs = (P(("sp", "tp"), None), P("tp", None, "sp"))
    return jax.shard_map(
        on_device, mesh=mesh, in_specs=in_specs, out_specs=out_specs, check_vma=False
    )
```

```python
import functools

import jax
import jax.numpy as jnp
from jax import lax
from jax.experimental import pallas as pl
from jax.experimental.pallas import tpu as pltpu
from jax.sharding import PartitionSpec as P

NZ, NX, NY = 8, 4, 4
GROUP = 64
LOG2E = 1.4426950408889634
LN2 = 0.6931471805599453
NEG = -1e30
eps = 1e-06


MESH = pl.DeviceIdType.MESH
SLOTS = 8


def fused_kernel(
    general,
    x_ref,
    ngain_ref,
    qgain_ref,
    kgain_ref,
    wq_ref,
    wk_ref,
    wv_ref,
    wb_ref,
    wc_ref,
    wi_ref,
    taps_ref,
    cgain_ref,
    w_att,
    w_conv,
    lam_ref,
    gain_ref,
    out_ref,
    log_out,
    xbuf,
    weights,
    gains,
    k_loc,
    v_loc,
    q_loc,
    u_loc,
    gate_loc,
    edge_buf,
    kbuf,
    vbuf,
    qbuf,
    wq,
    acc,
    lsum,
    stats,
    stats_in,
    part,
    part_in,
    heads,
    logs,
    conv_loc,
    a_in,
    cv_in,
    w_own,
    w_in,
    padded,
    a_rows,
    tops,
    s_send,
    s_recv,
    local_sem,
):
    f32, bf16 = jnp.float32, jnp.bfloat16
    sp = lax.axis_index("sp")
    y = lax.axis_index("tp")
    z = sp // (2 * NX)
    x = lax.rem(sp // 2, NX)
    c = lax.rem(sp, 2)
    zr = NZ - 1 - z
    rows = 512

    def dev(zz, xx, cc, yy):
        return ((zz * NX + xx) * 2 + cc, yy)

    def wrap(v, n):
        return lax.rem(v + n, n)

    z_up, z_dn = wrap(z + 1, NZ), wrap(z - 1, NZ)
    x_up, x_dn = dev(z, wrap(x + 1, NX), c, y), dev(z, wrap(x - 1, NX), c, y)
    up, dn = wrap(y + 1, NY), wrap(y - 1, NY)
    y_up, y_dn = dev(z, x, c, up), dev(z, x, c, dn)
    partner = dev(z, x, 1 - c, y)
    after, before = wrap(sp + 1, NZ * NX * 2), wrap(sp - 1, NZ * NX * 2)

    p_loads = [
        pltpu.make_async_copy(ref, weights.at[i], local_sem.at[i])
        for i, ref in enumerate((wk_ref, wv_ref, wq_ref, wc_ref, wi_ref, wb_ref))
    ]
    for copy in p_loads:
        copy.start()
    w_loads = [
        pltpu.make_async_copy(w_att, w_own.at[0], local_sem.at[6]),
        pltpu.make_async_copy(w_conv, w_own.at[1], local_sem.at[7]),
    ]
    for copy in w_loads:
        copy.start()

    barrier = pltpu.get_barrier_semaphore()
    peers = [dev(zz, x, cc, y) for zz in (z_up, z_dn) for cc in (c, 1 - c)]
    peers += [(after, y), (before, y)]
    peers += [dev(z, wrap(x + r, NX), c, y) for r in range(1, NX)]
    for o in range(NY):
        yy = wrap(y + o, NY)
        if o:
            peers.append(dev(z, x, c, yy))
        peers.append(dev(z, x, 1 - c, yy))
        peers.append(dev(zr, x, c, yy))
        peers.append(dev(zr, x, 1 - c, yy))
    for peer in peers:
        pl.semaphore_signal(barrier, inc=1, device_id=peer, device_id_type=MESH)

    own = x_ref.shape[0]
    piece = 16

    def norm(i, carry):
        at = pl.ds(pl.multiple_of(i * piece, piece), piece)
        v = x_ref[at].astype(f32)
        scale = lax.rsqrt(jnp.mean(v * v, axis=1, keepdims=True) + eps)
        xbuf[y, at] = (v * scale * ngain_ref[...]).astype(bf16)
        return carry

    lax.fori_loop(0, own // piece, norm, 0)
    for i, (ref, scale) in enumerate(((qgain_ref, 0.125), (kgain_ref, 1.0))):
        row = jnp.concatenate([ref[0:1], ref[1:2]], axis=1) * scale
        gains[i] = jnp.broadcast_to(row, (128, 128)).T
    pl.semaphore_wait(barrier, len(peers))

    numbers = [0]

    def new(count=1):
        numbers[0] += count
        return numbers[0] - count

    def remote(n, src, dst, to, m=None):
        return pltpu.make_async_remote_copy(
            src_ref=src,
            dst_ref=dst,
            send_sem=s_send.at[n],
            recv_sem=s_recv.at[n if m is None else m],
            device_id=to,
            device_id_type=MESH,
        )

    STAT, PART, HOME, LOGS, CONV, WY, WF, WC = (
        new(3), new(4), new(8), new(2), new(3), new(4), new(2), new(6)
    )

    half = own // 2

    def x_part(s, h):
        return xbuf.at[s, pl.ds(h * half, half)]

    x_one = [
        remote(new(), x_part(y, 0), x_part(y, 0), y_up),
        remote(new(), x_part(y, 1), x_part(y, 1), y_dn),
        remote(new(), x_part(y, 1), x_part(y, 1), y_up),
        remote(new(), x_part(y, 0), x_part(y, 0), y_dn),
    ]
    for copy in x_one:
        copy.start()
    x_far = [
        remote(new(), x_part(dn, 0), x_part(dn, 0), y_up),
        remote(new(), x_part(up, 1), x_part(up, 1), y_dn),
    ]
    edge = remote(new(), u_loc.at[pl.ds(rows - 16, 16)], edge_buf, (after, y))

    slots_y = [y, dn, up, wrap(y + 2, NY)]
    last = NZ // 2
    both_cores = pl.ds(0, 2)

    def k_at(slot, core, s):
        return kbuf.at[slot, core, pl.ds(pl.multiple_of(s * 128, 128), 128)]

    def v_at(slot, core, s):
        return vbuf.at[slot, core, s]

    at_of = (k_at, v_at)
    swaps, hop_one, hop_in, hops, q_one, q_two, q_x, q_far = [], [], [], {}, [], [], [], []
    q_to = dev(jnp.where(c == 0, z, zr), x, 1 - c, y)
    for i, s in enumerate(slots_y):
        swap, sends, waits = [], [], []
        for kv in range(2):
            if kv == 0:
                src = [k_loc.at[h, pl.ds(pl.multiple_of(s * 128, 128), 128)] for h in range(2)]
                other = k_loc.at[1 - c, pl.ds(pl.multiple_of(s * 128, 128), 128)]
            else:
                src = [v_loc.at[h, s] for h in range(2)]
                other = v_loc.at[1 - c, s]
            swap.append(remote(new(), other, at_of[kv](0, c, s), partner))
            for zz, slot in ((z_up, 1), (z_dn, SLOTS - 1)):
                n = new(2)
                for h in range(2):
                    sends.append(
                        remote(n + h, src[h], at_of[kv](slot, c, s), dev(zz, x, h, y), n + c)
                    )
                    waits.append(
                        remote(n + h, src[h], at_of[kv](slot, h, s), partner, n + h)
                    )
            for d in range(2, last + 1):
                for zz, a, b, core in (
                    (z_up, d - 1, d, 0),
                    (z_dn, SLOTS - d + 1, SLOTS - d, 1),
                ):
                    pick = both_cores if d < last else core
                    hops.setdefault((d, i), []).append(
                        remote(new(), at_of[kv](a, pick, s), at_of[kv](b, pick, s), dev(zz, x, c, y))
                    )
        swaps.append(swap)
        hop_one.append(sends)
        hop_in.append(waits)
        q_one.append(remote(new(), q_loc.at[1 - c, s], qbuf.at[c, s], q_to))
        q_two.append(remote(new(), q_loc.at[1, s], qbuf.at[1, s], dev(zr, x, 1, y)))
        pair = pl.ds(0, 2)
        q_x.append(
            [
                remote(new(), qbuf.at[pair, s], qbuf.at[pl.ds(2, 2), s], x_dn),
                remote(new(), qbuf.at[pair, s], qbuf.at[pl.ds(6, 2), s], x_up),
            ]
        )
        q_far.append(
            [
                remote(new(), qbuf.at[2, s], qbuf.at[4, s], x_dn),
                remote(new(), qbuf.at[7, s], qbuf.at[5, s], x_up),
            ]
        )
    assert numbers[0] <= s_send.shape[0]

    def w_half(kind, cc):
        return w_own.at[kind, pl.ds(cc * 128, 128)]

    def w_slot(d, kind, cc):
        return w_in.at[d - 1, kind, pl.ds(cc * 128, 128)]

    w_first = [
        remote(WY, w_half(0, c), w_slot(1, 0, c), y_up),
        remote(WY + 1, w_half(1, c), w_slot(1, 1, c), y_up),
        remote(WY + 2, w_half(0, c), w_slot(3, 0, c), y_dn),
        remote(WY + 3, w_half(1, c), w_slot(3, 1, c), y_dn),
    ]
    w_far = [
        remote(WF, w_slot(1, 0, c), w_slot(2, 0, c), y_up),
        remote(WF + 1, w_slot(3, 1, c), w_slot(2, 1, c), y_dn),
    ]
    w_core = [
        remote(WC + 2 * (d - 1) + kind, w_slot(d, kind, c), w_slot(d, kind, c), partner)
        for d in range(1, NY)
        for kind in range(2)
    ]
    convs = [
        remote(
            CONV + o - 1,
            conv_loc.at[wrap(y + o, NY)],
            cv_in.at[o],
            dev(z, x, c, wrap(y + o, NY)),
        )
        for o in range(1, NY)
    ]
    cv_own = pltpu.make_async_copy(conv_loc.at[y], cv_in.at[0], local_sem.at[3])

    def body(s_acc, o_acc):
        def project(s):
            at = pl.ds(pl.multiple_of(s * own, own), own)
            out = []
            for n in range(6):
                j = n % 2
                for t in range(8):
                    pltpu.matmul_push_rhs(
                        weights[n, t * 256 : (t + 1) * 256], staging_register=0, mxu_index=j
                    )
                    pltpu.matmul_acc_lhs(
                        o_acc[j], xbuf[s, :, t * 256 : (t + 1) * 256], load_staged_rhs=0
                    )
                out.append(pltpu.matmul_pop(o_acc[j]).astype(bf16).astype(f32))

            def scaled(v):
                r = v.T.reshape(4, 64, own)
                r = r * lax.rsqrt(jnp.mean(r * r, axis=1, keepdims=True) + eps)
                return r.reshape(2, 128, own)

            k = scaled(out[0])
            k = [(k[h] * gains[1]).T.astype(bf16) for h in range(2)]
            v = out[1].T.astype(bf16)
            v = [v[:128], v[128:]]
            q = scaled(out[2])
            for h in range(2):
                k_loc[h, at] = k[h]
                v_loc[h, s] = v[h]
                q_loc[h, s] = (q[h] * gains[0]).astype(bf16)

                @pl.when(c == h)
                def _(h=h):
                    kbuf[0, h, at] = k[h]
                    vbuf[0, h, s] = v[h]

            @pl.when(c == 0)
            def _():
                qbuf[0, s] = (q[0] * gains[0]).astype(bf16)

            u_loc[at] = (out[3] * out[4]).astype(bf16)
            gate_loc[at] = out[5].astype(bf16)

            @pl.when(s == NY - 1)
            def _():
                edge.start()

        def launch(i):
            for copy in hop_one[i] + swaps[i]:
                copy.start()
            q_one[i].start()

            @pl.when(c == 1)
            def _():
                q_two[i].start()

        def second(i):
            q_one[i].wait_recv()

            @pl.when(c == 1)
            def _():
                q_two[i].wait_recv()

            for copy in q_x[i]:
                copy.start()
            for copy in hop_in[i]:
                copy.wait_recv()
            for copy in hops[2, i]:
                copy.start()

        def relay(i):
            for copy in q_x[i]:
                copy.wait_recv()
            for copy in q_far[i]:
                copy.start()

        def third(i):
            for copy in hops[2, i]:
                copy.wait_recv()
            for copy in hops[3, i]:
                copy.start()

        def fourth(i):
            for copy in hops[3, i]:
                copy.wait_recv()
            for copy in hops[4, i]:
                copy.start()

        for copy in p_loads:
            copy.wait()
        project(slots_y[0])
        launch(0)
        x_one[0].wait_recv()
        x_far[0].start()
        x_one[1].wait_recv()
        x_far[1].start()
        second(0)
        wq[...] = jnp.zeros(wq.shape, bf16)
        acc[...] = jnp.zeros(acc.shape, f32)
        lsum[...] = jnp.zeros(lsum.shape, f32)
        tops[...] = jnp.full(tops.shape, NEG, f32)
        x_one[2].wait_recv()
        project(slots_y[1])
        launch(1)
        x_one[3].wait_recv()
        project(slots_y[2])
        launch(2)
        relay(0)
        third(0)
        second(1)
        for copy in x_far:
            copy.wait_recv()
        project(slots_y[3])
        launch(3)
        for copy in w_loads:
            copy.wait()
        for copy in w_first:
            copy.start()
        second(2)
        fourth(0)
        relay(1)
        third(1)

        edge.wait_recv()
        width = u_loc.shape[1]
        padded[8:] = u_loc[...].astype(f32)
        padded[:8] = jnp.where(sp == 0, 0.0, edge_buf[8:].astype(f32))
        group = lax.broadcasted_iota(jnp.int32, (width, width), 0) // GROUP
        same = group == lax.broadcasted_iota(jnp.int32, (width, width), 1) // GROUP
        mean_of = jnp.where(same, 1.0 / GROUP, 0.0).astype(bf16)

        def conv_block(i, carry):
            at = pl.multiple_of(i * 128, 128)
            window = padded[pl.ds(at, 136)]
            conv = taps_ref[0:1] * window[6:134]
            conv += taps_ref[1:2] * window[7:135]
            conv += taps_ref[2:3] * window[8:136]
            gated = gate_loc[pl.ds(at, 128)].astype(f32) * conv
            square = gated * gated
            high = square.astype(bf16)
            low = (square - high.astype(f32)).astype(bf16)
            pltpu.matmul_push_rhs(mean_of, staging_register=0, mxu_index=0)
            pltpu.matmul_acc_lhs(o_acc[0], high, load_staged_rhs=0)
            pltpu.matmul_acc_lhs(o_acc[0], low)
            mean = pltpu.matmul_pop(o_acc[0])
            conv_loc[i] = (gated * lax.rsqrt(mean + eps) * cgain_ref[...]).astype(bf16)
            return carry

        lax.fori_loop(0, NY, conv_block, 0)
        cv_own.start()
        for copy in convs:
            copy.start()
        second(3)
        relay(2)

        def prepare(t):
            for s in range(NY):
                cs = slice(s * 128, (s + 1) * 128)
                for m in range(2):
                    q = qbuf[t, s, 64 * m : 64 * m + 64].astype(f32) * LOG2E
                    high = q.astype(bf16)
                    wq[t, m, 64 * m : 64 * m + 64, cs] = high
                    wq[t, m, 128 + 64 * m : 192 + 64 * m, cs] = (q - high.astype(f32)).astype(bf16)

        def prepare_all(lo, hi):
            def each(i, carry):
                prepare(i)
                return carry

            lax.fori_loop(lo, hi, each, 0)

        for swap in swaps:
            for copy in swap:
                copy.wait_recv()

        def q_start(t):
            r, h = t // 2, lax.rem(t, 2)
            zq = jnp.where(h == 0, z, zr)
            return ((zq * NX + wrap(x + r, NX)) * 2 + h) * rows

        def v_chunk(s, g):
            a = 2 * (g % 2)
            return jnp.concatenate([vbuf[s, g // 2, a], vbuf[s, g // 2, a + 1]], axis=1)

        def run(t, slots, masked, diff):
            its = [(s, m, g) for m in range(2) for s in slots for g in range(4)]
            n = len(its)
            lag, bufs = 2, 3

            def start(i):
                s, m, g = its[i]
                k = kbuf[s, g // 2, (g % 2) * 256 : (g % 2) * 256 + 256]
                lhs = jnp.concatenate([k, k], axis=1)
                for j in range(2):
                    pltpu.matmul_push_rhs(
                        wq[t, m, :, j * 256 : (j + 1) * 256], staging_register=0, mxu_index=j
                    )
                    pltpu.matmul_acc_lhs(s_acc[j][i % bufs], lhs, load_staged_rhs=0)

            def drain(i, j):
                g = its[i][2]
                sc = pltpu.matmul_pop(s_acc[j][i % bufs])
                if masked:
                    d = lax.broadcasted_iota(jnp.int32, sc.shape, 0) - lax.broadcasted_iota(
                        jnp.int32, sc.shape, 1
                    )
                    sc = jnp.where(d <= diff + (j * 256 - g * 256), sc, NEG)
                return sc

            shift = {}
            if general:
                best = {}
                for i in range(lag):
                    start(i)
                for i in range(n):
                    if i + lag < n:
                        start(i + lag)
                    for j in range(2):
                        top = jnp.max(drain(i, j).reshape(32, 8, 256), axis=0)
                        key = (its[i][1], j)
                        best[key] = jnp.maximum(best[key], top) if key in best else top
                for (m, j), top in best.items():
                    cs = slice(j * 256, (j + 1) * 256)
                    before = tops[t, m : m + 1, cs]
                    now = jnp.maximum(before, jnp.max(top, axis=0, keepdims=True))
                    tops[t, m : m + 1, cs] = now
                    fade = jnp.exp2(before - now)
                    acc[t, m, :, cs] = acc[t, m, :, cs] * fade
                    lsum[t, m, :, cs] = lsum[t, m, :, cs] * fade
                    shift[m, j] = now

            ls = [None, None]
            for i in range(lag):
                start(i)
            for i in range(n):
                s, m, g = its[i]
                if i + lag < n:
                    start(i + lag)
                for j in range(2):
                    sc = drain(i, j)
                    p = jnp.exp2(sc - shift[m, j] if general else sc)
                    one = jnp.sum(p.reshape(32, 8, 256), axis=0)
                    ls[j] = one if ls[j] is None else ls[j] + one
                    pltpu.matmul_push_rhs(p.astype(bf16), staging_register=1, mxu_index=j)
                    pltpu.matmul_acc_lhs(
                        o_acc[j],
                        v_chunk(s, g),
                        load_staged_rhs=1,
                    )
                if i + 1 == n or its[i + 1][1] != m:
                    for j in range(2):
                        cs = slice(j * 256, (j + 1) * 256)
                        acc[t, m, :, cs] += pltpu.matmul_pop(o_acc[j])
                        lsum[t, m, :, cs] += ls[j]
                    ls = [None, None]

        def step(u, carry):
            @pl.when(u == 3)
            def _():
                for copy in w_first:
                    copy.wait_recv()
                for copy in w_far + w_core[:2] + w_core[4:]:
                    copy.start()

            @pl.when(u == last)
            def _():
                for i in range(NY):
                    for copy in hops[last, i]:
                        copy.wait_recv()

            sa, sb = u, lax.rem(SLOTS - u, SLOTS)
            two = (u > 0) & (u < last)

            def tile(i, carry):
                t = jnp.where(i < 4, i, jnp.where(i < 6, i + 2, i - 2))

                @pl.when((u == 0) & (i == 0))
                def _():
                    prepare_all(0, 2)

                @pl.when((u == 0) & (i == 2))
                def _():
                    relay(3)
                    prepare_all(2, 4)
                    prepare_all(6, 8)

                @pl.when((u == 0) & (i == 3))
                def _():
                    third(2)

                @pl.when((u == 0) & (i == 5))
                def _():
                    third(3)

                @pl.when((u == 0) & (i == 6))
                def _():
                    for copies in q_far:
                        for copy in copies:
                            copy.wait_recv()
                    prepare_all(4, 6)
                    fourth(1)

                @pl.when((u == 1) & (i == 0))
                def _():
                    fourth(2)

                @pl.when((u == 1) & (i == 3))
                def _():
                    fourth(3)

                def diff_of(s):
                    zk = wrap(z - s, NZ)
                    return q_start(t) - (zk * NX + x) * 2 * rows

                da, db = diff_of(sa), diff_of(sb)
                full = 2 * rows
                both = two & (da >= full) & (db >= full)

                @pl.when(both)
                def _():
                    run(t, [sa, sb], False, 0)

                @pl.when(jnp.logical_not(both))
                def _():
                    def one(b, carry):
                        s = jnp.where(b == 0, sa, sb)
                        diff = diff_of(s)

                        @pl.when(diff >= full)
                        def _():
                            run(t, [s], False, 0)

                        @pl.when((diff >= 0) & (diff < full))
                        def _():
                            run(t, [s], True, diff)

                        return carry

                    lax.fori_loop(0, jnp.where(two, 2, 1), one, 0)

                return carry

            lax.fori_loop(0, 2 * NX, tile, 0)
            return carry

        lax.fori_loop(0, last + 1, step, 0)

        for t in range(2 * NX):
            for m in range(2):
                stats[t, m : m + 1] = jnp.sum(lsum[t, m], axis=0, keepdims=True)
            if general:
                stats[t, 2:4] = tops[t]
        st = [
            remote(STAT + r - 1, stats, stats_in.at[r - 1], dev(z, wrap(x - r, NX), c, y))
            for r in range(1, NX)
        ]
        for copy in st:
            copy.start()
        for copy in st:
            copy.wait_recv()
        lam = lam_ref[c]

        def parts_of(t):
            return [stats[t]] + [stats_in[r - 1, (t - 2 * r) % (2 * NX)] for r in range(1, NX)]

        def total(t):
            each = parts_of(t)
            if not general:
                return each[0] + each[1] + each[2] + each[3], 0.0
            top = functools.reduce(jnp.maximum, [e[2:4] for e in each])
            return sum(e[0:2] * jnp.exp2(e[2:4] - top) for e in each), top

        def partial(t):
            tot, top = total(t)
            own = jnp.exp2(tops[t] - top) if general else jnp.ones_like(tot)
            return acc[t, 0] * (own[0:1] / tot[0:1]) - acc[t, 1] * (lam * own[1:2] / tot[1:2])

        def log_total(t):
            tot, top = total(t)
            return jnp.log(tot) + top * LN2

        part[4] = partial(4).astype(bf16)
        part[5] = partial(5).astype(bf16)
        p_far = [
            remote(PART, part.at[4], part_in.at[0], x_up),
            remote(PART + 1, part.at[5], part_in.at[1], x_dn),
        ]
        for copy in p_far:
            copy.start()
        for t in (2, 3, 6, 7, 0, 1):
            acc[t, 0] = partial(t)
        for h in range(2):
            logs[h] = log_total(h)
        part[3] = acc[3, 0].astype(bf16)
        part[6] = acc[6, 0].astype(bf16)
        for copy in w_far:
            copy.wait_recv()
        for copy in w_core[2:4]:
            copy.start()
        for copy in p_far:
            copy.wait_recv()
        part[2] = (acc[2, 0] + part_in[0].astype(f32)).astype(bf16)
        part[7] = (acc[7, 0] + part_in[1].astype(f32)).astype(bf16)
        p_near = [
            remote(PART + 2, part.at[pl.ds(2, 2)], part_in.at[pl.ds(2, 2)], x_up),
            remote(PART + 3, part.at[pl.ds(6, 2)], part_in.at[pl.ds(4, 2)], x_dn),
        ]
        for copy in p_near:
            copy.start()
        for copy in p_near:
            copy.wait_recv()

        gain = jnp.broadcast_to(gain_ref[...], (128, 128)).T
        gain = jnp.concatenate([gain] * NY, axis=1)
        for h in range(2):
            attn = acc[h, 0] + part_in[2 + h].astype(f32) + part_in[4 + h].astype(f32)
            mean = jnp.mean(attn * attn, axis=0, keepdims=True)
            heads_t = (attn * lax.rsqrt(mean + eps) * gain).astype(bf16)
            for yy in range(NY):
                heads[h, yy] = heads_t[:, yy * 128 : (yy + 1) * 128]
        zh = (z, zr)
        own_head = pltpu.make_async_copy(heads.at[0, y], a_in.at[0], local_sem.at[4])
        own_log = pltpu.make_async_copy(logs.at[0], log_out.at[c], local_sem.at[5])
        late = []
        for h in range(2):
            for o in range(NY):
                yy = wrap(y + o, NY)
                copy = pltpu.make_async_remote_copy(
                    src_ref=heads.at[h, yy],
                    dst_ref=a_in.at[2 * o + c],
                    send_sem=s_send.at[HOME + 4 * h + o],
                    recv_sem=s_recv.at[HOME + 2 * o + c],
                    device_id=dev(zh[h], x, h, yy),
                    device_id_type=MESH,
                )
                if h == 0 and o == 0:
                    first = copy
                else:
                    copy.start()
                    late.append(copy)
            copy = pltpu.make_async_remote_copy(
                src_ref=logs.at[h],
                dst_ref=log_out.at[c],
                send_sem=s_send.at[LOGS + h],
                recv_sem=s_recv.at[LOGS + c],
                device_id=dev(zh[h], x, h, y),
                device_id_type=MESH,
            )
            if h == 0:
                first_log = copy
            else:
                copy.start()
                late.append(copy)

        @pl.when(c == 0)
        def _():
            own_head.start()
            own_log.start()

        @pl.when(c == 1)
        def _():
            first.start()
            first_log.start()

        for copy in w_core + convs:
            copy.wait()
        cv_own.wait()

        def product(n, lhs_of, kind):
            out = []
            for j in range(2):
                at = pl.ds(pl.multiple_of((2 * n + j) * 256, 256), 256)
                for d in range(NY):
                    w = w_own[kind, :, at] if d == 0 else w_in[d - 1, kind, :, at]
                    pltpu.matmul_push_rhs(w, staging_register=0, mxu_index=j)
                    pltpu.matmul_acc_lhs(o_acc[j], lhs_of(d), load_staged_rhs=0)
                out.append((at, pltpu.matmul_pop(o_acc[j])))
            return out

        def conv_out_part(n, carry):
            for at, value in product(n, lambda d: cv_in[d], 1):
                out_ref[:, at] = value
            return carry

        lax.fori_loop(0, out_ref.shape[1] // 512, conv_out_part, 0)

        for s in range(2 * NY):

            @pl.when((c == 1) | (s > 0))
            def _(s=s):
                remote(HOME, heads.at[0, 0], a_in.at[s], partner, HOME + s).wait_recv()

        @pl.when(c == 0)
        def _():
            own_head.wait()
            own_log.wait()

        for s in range(2 * NY):
            a_rows[:, s * 128 : (s + 1) * 128] = a_in[s].T

        def head_out_part(n, carry):
            for at, value in product(n, lambda d: a_rows[:, d * 256 : (d + 1) * 256], 0):
                out_ref[:, at] += value
            return carry

        lax.fori_loop(0, out_ref.shape[1] // 512, head_out_part, 0)

        sent = x_one + x_far + [edge] + st + p_far + p_near + late + w_first + w_far + q_one
        for i in range(NY):
            sent += swaps[i] + hop_one[i] + q_x[i] + q_far[i]
            for d in range(2, last + 1):
                sent += hops[d, i]
        for copy in sent:
            copy.wait_send()

        @pl.when(c == 1)
        def _():
            for copy in q_two:
                copy.wait_send()

        for s in range(2):

            @pl.when((c == 1) | (s == 1))
            def _(s=s):
                remote(LOGS, logs.at[0], log_out.at[s], partner, LOGS + s).wait_recv()

        @pl.when(c == 1)
        def _():
            first.wait_send()
            first_log.wait_send()

    def made(q, count):
        return pltpu.ACC(q)((count, 256), f32)

    pl.run_scoped(
        body, [[made(q, 256) for _ in range(3)] for q in range(2)], [made(q, 128) for q in range(2)]
    )


def fused(general, inputs, *others):
    f32, bf16 = jnp.float32, jnp.bfloat16
    own, model = inputs.shape
    w_att = others[11]
    rows, channels, width = own * NY, w_att.shape[0], w_att.shape[1]
    vm = pl.BlockSpec(memory_space=pltpu.VMEM)
    hbm = pl.BlockSpec(memory_space=pltpu.HBM)
    sm = pl.BlockSpec(memory_space=pltpu.SMEM)
    tiles = 2 * NX
    count = 160
    return pl.pallas_call(
        functools.partial(fused_kernel, general),
        in_specs=[vm] * 4 + [hbm] * 6 + [vm, vm, hbm, hbm, sm, vm],
        out_specs=[vm, vm],
        out_shape=[
            jax.ShapeDtypeStruct((own, width), f32),
            jax.ShapeDtypeStruct((2, 2, rows), f32),
        ],
        scratch_shapes=[
            pltpu.VMEM((NY, own, model), bf16),
            pltpu.VMEM((6, model, channels), bf16),
            pltpu.VMEM((2, 128, 128), f32),
            pltpu.VMEM((2, rows, 128), bf16),
            pltpu.VMEM((2, NY, 128, 128), bf16),
            pltpu.VMEM((2, NY, 128, 128), bf16),
            pltpu.VMEM((rows, channels), bf16),
            pltpu.VMEM((rows, channels), bf16),
            pltpu.VMEM((16, channels), bf16),
            pltpu.VMEM((SLOTS, 2, rows, 128), bf16),
            pltpu.VMEM((SLOTS, 2, NY, 128, 128), bf16),
            pltpu.VMEM((tiles, NY, 128, 128), bf16),
            pltpu.VMEM((tiles, 2, 256, rows), bf16),
            pltpu.VMEM((tiles, 2, 128, rows), f32),
            pltpu.VMEM((tiles, 2, 8, rows), f32),
            pltpu.VMEM((tiles, 4 if general else 2, rows), f32),
            pltpu.VMEM((NX - 1, tiles, 4 if general else 2, rows), f32),
            pltpu.VMEM((tiles, 128, rows), bf16),
            pltpu.VMEM((6, 128, rows), bf16),
            pltpu.VMEM((2, NY, 128, 128), bf16),
            pltpu.VMEM((2, 2, rows), f32),
            pltpu.VMEM((NY, own, channels), bf16),
            pltpu.VMEM((2 * NY, 128, 128), bf16),
            pltpu.VMEM((NY, own, channels), bf16),
            pltpu.VMEM((2, *w_att.shape), bf16),
            pltpu.VMEM((NY - 1, 2, *w_att.shape), bf16),
            pltpu.VMEM((rows + 8, channels), f32),
            pltpu.VMEM((own, NY * 256), bf16),
            pltpu.VMEM((tiles, 2, rows), f32),
            pltpu.SemaphoreType.DMA((count,)),
            pltpu.SemaphoreType.DMA((count,)),
            pltpu.SemaphoreType.DMA((8,)),
        ],
        cost_estimate=pl.CostEstimate(
            flops=2 * 10**10, bytes_accessed=16 * 2**20, transcendentals=34 * 10**6
        ),
        compiler_params=pltpu.CompilerParams(
            collective_id=1 if general else 0,
            has_side_effects=True,
            vmem_limit_bytes=63 * 1024 * 1024,
        ),
    )(inputs, *others)


def on_device(
    inputs,
    norm_gain,
    w_query,
    w_key,
    w_value,
    query_gain,
    key_gain,
    lambdas,
    sub_gain,
    w_gate_b,
    w_gate_c,
    w_conv_in,
    conv_taps,
    conv_gain,
    w_out_att,
    w_out_conv,
):
    comp = query_gain.shape[1]
    reach = jnp.max(jnp.abs(query_gain * key_gain)) * (comp**0.5) * LOG2E * 1.02
    return tuple(
        lax.cond(
            reach < 90.0,
            functools.partial(fused, False),
            functools.partial(fused, True),
            inputs,
            norm_gain[None],
            query_gain,
            key_gain,
            w_query,
            w_key,
            w_value,
            w_gate_b,
            w_gate_c,
            w_conv_in,
            conv_taps,
            conv_gain[None],
            w_out_att,
            w_out_conv,
            lambdas,
            sub_gain[None],
        )
    )


def solution(mesh):
    in_specs = (
        P(("sp", "tp"), None),
        P(),
        P(None, "tp"),
        P(None, "tp"),
        P(None, "tp"),
        P(),
        P(),
        P("tp"),
        P(),
        P(None, "tp"),
        P(None, "tp"),
        P(None, "tp"),
        P(None, "tp"),
        P("tp"),
        P("tp", None),
        P("tp", None),
    )
    out_specs = (P(("sp", "tp"), None), P("tp", None, "sp"))
    return jax.shard_map(
        on_device, mesh=mesh, in_specs=in_specs, out_specs=out_specs, check_vma=False
    )
```
